32 devices in a mesh: ep: 8 (over z, core), tp: 4 (over y, x).
Axes of the slice: x: 2, y: 2, z: 4, core: 2. Of those that a mesh axis runs over, the one named last changes fastest.
Arguments:
- mixer_input: bfloat16 [2048, 2048], P('ep'), may hold values from -6 to 6
- mixer_gain: float32 [2048], replicated, may hold values from 0.1 to 1.9
- query_weight: bfloat16 [2048, 2048], P(None, 'tp'), may hold values from -0.13258252 to 0.13258252
- key_weight: bfloat16 [2048, 1024], P(None, 'tp'), may hold values from -2.78423295 to 2.78423295
- value_weight: bfloat16 [2048, 1024], P(None, 'tp'), may hold values from -0.125 to 0.125
- output_weight: bfloat16 [2048, 2048], P(None, 'tp'), may hold values from -1 to 1
- sink_logit: float32 [32], P('tp'), may hold values from 2 to 7
- expert_input: bfloat16 [1024, 2048], P('ep'), may hold values from -6 to 6
- expert_gain: float32 [2048], replicated, may hold values from 0.1 to 1.9
- routes: int32 [1024, 4], P('ep'), may hold values from 0 to 7, all different within a row; in each aligned block of 128 rows (0 to 127, 128 to 255, ...) at most 128 rows name the same one
- route_logits: float32 [1024, 4], P('ep'), may hold values from -6 to 6
- gate_weight: bfloat16 [8, 2048, 2048], P('ep', None, 'tp'), may hold values from -0.375 to 0.375
- up_weight: bfloat16 [8, 2048, 2048], P('ep', None, 'tp'), may hold values from -0.375 to 0.375
- down_weight: bfloat16 [8, 2048, 2048], P('ep', None, 'tp'), may hold values from -0.03125 to 0.03125
Outputs:
- mixer_output: bfloat16 [2048, 2048], P('ep', 'tp')
- expert_output: bfloat16 [1024, 2048], P('ep', 'tp')
The draws below stay inside these ranges and needn't reach their ends.
Inputs may be any that keep to these rules, and one draw needn't show every extreme that they name: `routes`: each token names 4 different experts. Among the 128 tokens of one index of ep (aligned blocks) no expert is named more than 128 times, and in some blocks one expert is named exactly 128 times.
All inputs are finite; a program needn't handle non-finite values.
Results may differ from the reference program's by a relative error of at most 0.0055.
The reference program's roundings to bfloat16 on the way count: a program that leaves them out, or rounds other values in their place, can miss the bound.
Values may be sent and summed in bfloat16 or wider, within the bound.
A program may use at most 64 MiB of HBM per device.

```python
import math
import jax
import jax.numpy as jnp
import numpy as np
from jax import lax

D = 2048
HEADS = 32
KV_HEADS = 16
HEAD_DIM = 64
FF = 2048
TOP_K = 4
WINDOW = 128
GRID_W = 64
EXP_DEV = 128
EXPERTS = 8
CAP = 128
MIX_TOKENS = 2048
EXP_TOKENS = 1024
N_EP = 8


def paired_weights(key):
    base = jax.random.fold_in(key, 11)
    first, second = jax.random.split(base)
    query = jnp.clip(jax.random.normal(first, (D, HEADS * HEAD_DIM), jnp.float32), -6.0, 6.0) / math.sqrt(D)
    noise = jnp.clip(jax.random.normal(second, (D, KV_HEADS * HEAD_DIM), jnp.float32), -6.0, 6.0) / math.sqrt(D)
    keys = noise
    return (query, keys)


def draw_query_weight(key, part):
    return paired_weights(key)[0].astype(jnp.bfloat16)


def draw_key_weight(key, part):
    return paired_weights(key)[1].astype(jnp.bfloat16)


def levels(rng, shape, pieces, least, largest):
    level = 1.0
    for position, blocks in pieces:
        draws = jax.random.uniform(jax.random.fold_in(jax.random.fold_in(rng, 6), position), (blocks,), jnp.float32, least / len(pieces), largest / len(pieces))
        level = level * jnp.repeat(jnp.exp(draws), shape[position] // blocks).reshape((-1,) + (1,) * (len(shape) - 1 - position))
    return level


def routed_block(own_key, own, number, rows, amount, top, reach, slope):
    sequence = jax.random.permutation(own_key, amount)
    packed, common = portions_of(amount, rows * top, reach, slope, True), portions_of(amount, rows * top, reach, slope, False)
    places = jnp.arange(amount)

    def named(sizes, rotation):
        used = int((sizes > 0).sum())
        fixed = max(1, used // 4)
        moved = fixed + (places - fixed + rotation * (used - fixed)) % max(1, amount - fixed)
        return jnp.zeros((amount,), jnp.int32).at[sequence[jnp.where(places < fixed, places, moved)]].set(jnp.asarray(sizes, jnp.int32))

    sizes = jnp.where(number % 4 == 0, named(packed, number // 4), named(common, number - number // 4 - 1))
    mixed = jax.random.permutation(jax.random.fold_in(own, 3), amount)
    giver, sink = mixed[0:amount // 2 * 2:2], mixed[1:amount // 2 * 2:2]
    margin = jnp.minimum(sizes[giver] - 1, reach - sizes[sink]) // 2
    margin = jnp.where((giver == sequence[0]) | (sink == sequence[0]) | (sizes[sink] == 0), 0, jnp.maximum(margin, 0))
    moved = jax.random.randint(jax.random.fold_in(own, 4), (amount // 2,), 0, 1 << 20) % (margin + 1)
    sizes = sizes.at[giver].add(-moved).at[sink].add(moved)
    labels = jnp.searchsorted(jnp.cumsum(sizes), jnp.arange(rows * top), side="right").astype(jnp.int32)
    grid = labels.reshape(top, rows).T
    grid = grid[jax.random.permutation(jax.random.fold_in(own, 1), rows)]
    rotation = jax.random.randint(jax.random.fold_in(own, 2), (rows, 1), 0, top)
    return jnp.take_along_axis(grid, (jnp.arange(top)[None, :] + rotation) % top, axis=1)


def portions_of(amount, total, reach, slope, full):
    portions = [(1 << 20) // math.isqrt(standing ** slope) + 1 for standing in range(1, amount + 1)]
    largest = reach if full else min(reach, max(-(-total // amount), total * portions[0] // sum(portions)))
    least = 1 if total - largest >= amount - 1 else 0
    given, rest = [largest] + [least] * (amount - 1), total - largest - least * (amount - 1)
    while rest > 0:
        free = [i for i in range(1, amount) if given[i] < largest] or [i for i in range(1, amount) if given[i] < reach]
        whole, remaining = sum([portions[i] for i in free]), rest
        for i in free:
            addition = min(reach - given[i], max(1, remaining * portions[i] // whole), rest)
            given[i] = given[i] + addition
            rest = rest - addition
    return np.array(given)


def gaussian(rng, extent, width, reach, cuts=(), kind=jnp.bfloat16):
    entries = jax.random.normal(rng, extent, jnp.float32) * width
    if len(cuts) > 0:
        entries = levels(rng, extent, cuts, -0.22, 0.18) * entries
    return jnp.clip(entries, min=-reach, max=reach).astype(kind)


def setup_inputs(seed: int = 0) -> dict:
    splits = jax.random.split(jax.random.key(seed), 15)
    mixer_input = gaussian(splits[0], (MIX_TOKENS, D), 1.0, 6.0, ((0, 8),))
    mixer_gain = jnp.clip(1.0 + 0.18 * jax.random.normal(splits[1], (D,), jnp.float32), 0.1, 1.9)
    query_weight = draw_query_weight(jax.random.fold_in(splits[14], 71), 0)
    key_weight = draw_key_weight(jax.random.fold_in(splits[14], 71), 0)
    value_weight = gaussian(splits[4], (D, KV_HEADS * HEAD_DIM), D ** -0.5, 0.125, ((1, 4),))
    output_weight = gaussian(splits[5], (HEADS * HEAD_DIM, D), (HEADS * HEAD_DIM // 64) ** -0.5, 1.0, ((1, 4),))
    sink_logit = jnp.clip(2.0 + 5.0 * jax.random.uniform(splits[6], (HEADS,), jnp.float32) ** levels(splits[6], (HEADS,), ((0, 4),), -0.2, 0.2), 2.0, 7.0)
    expert_input = gaussian(splits[7], (EXP_TOKENS, D), 1.0, 6.0, ((0, 8),))
    expert_gain = jnp.clip(1.0 + 0.18 * jax.random.normal(splits[8], (D,), jnp.float32), 0.1, 1.9)
    routes_keys = jax.random.split(jax.random.fold_in(splits[9], 1), EXP_TOKENS // EXP_DEV)
    routes_turns = jax.random.permutation(jax.random.fold_in(splits[9], 3), EXP_TOKENS // EXP_DEV)
    routes = jax.vmap(lambda own, number: routed_block(jax.random.fold_in(splits[9], 2), own, number, EXP_DEV, EXPERTS, TOP_K, CAP, 2))(routes_keys, routes_turns).reshape((EXP_TOKENS, TOP_K))
    route_logits = gaussian(splits[10], (EXP_TOKENS, TOP_K), 1.5, 6.0, ((0, 8),), jnp.float32)
    gate_weight = gaussian(splits[11], (EXPERTS, D, FF), (D // 9) ** -0.5, 0.375, ((0, 8), (2, 4)))
    up_weight = gaussian(splits[12], (EXPERTS, D, FF), (D // 9) ** -0.5, 0.375, ((0, 8), (2, 4)))
    down_weight = gaussian(splits[13], (EXPERTS, FF, D), (16 * FF) ** -0.5, 0.03125, ((0, 8), (2, 4)))
    return {"mixer_input": mixer_input, "mixer_gain": mixer_gain, "query_weight": query_weight, "key_weight": key_weight, "value_weight": value_weight, "output_weight": output_weight, "sink_logit": sink_logit, "expert_input": expert_input, "expert_gain": expert_gain, "routes": routes, "route_logits": route_logits, "gate_weight": gate_weight, "up_weight": up_weight, "down_weight": down_weight}


EPSILON = 1e-06
LIMIT = 7.0
SLOPE = 1.702
BASE = 10000.0

def normalize(rows, gain):
    values = rows.astype(jnp.float32)
    scaled = values * lax.rsqrt(lax.optimization_barrier(jnp.mean(values * values, axis=-1, keepdims=True)) + EPSILON)
    return (scaled * gain).astype(jnp.bfloat16)

def turn(values, cosine, sine):
    first, second = jnp.split(values, 2, axis=-1)
    cosine = cosine[:, None, :]
    sine = sine[:, None, :]
    return jnp.concatenate([first * cosine - second * sine, second * cosine + first * sine], axis=-1)

def axial_rope(values, places):
    quarter = values.shape[-1] // 4
    frequency = BASE ** (-jnp.arange(quarter, dtype=jnp.float32) / quarter)
    row_angle = (places // GRID_W).astype(jnp.float32)[:, None] * frequency[None, :]
    column_angle = (places % GRID_W).astype(jnp.float32)[:, None] * frequency[None, :]
    row_part, column_part = jnp.split(values, 2, axis=-1)
    return jnp.concatenate([turn(row_part, jnp.cos(row_angle), jnp.sin(row_angle)), turn(column_part, jnp.cos(column_angle), jnp.sin(column_angle))], axis=-1)

def activate(gate, up):
    capped = jnp.minimum(gate, LIMIT)
    bounded = jnp.clip(up, -LIMIT, LIMIT)
    return (capped * jax.nn.sigmoid(SLOPE * capped) * (bounded + 1.0)).astype(jnp.bfloat16)

def band_attention(parts):
    query, keys, values, sinks = parts
    total = query.shape[0]
    group = query.shape[1]
    blocks = total // WINDOW
    padded_keys = jnp.pad(keys, ((WINDOW, WINDOW), (0, 0))).reshape(blocks + 2, WINDOW, HEAD_DIM)
    padded_values = jnp.pad(values, ((WINDOW, WINDOW), (0, 0))).reshape(blocks + 2, WINDOW, HEAD_DIM)
    near_keys = jnp.concatenate([padded_keys[:-2], padded_keys[1:-1], padded_keys[2:]], axis=1)
    near_values = jnp.concatenate([padded_values[:-2], padded_values[1:-1], padded_values[2:]], axis=1)
    blocked = query.reshape(blocks, WINDOW, group, HEAD_DIM)
    scores = jnp.einsum('nqrd,nkd->nrqk', blocked.astype(jnp.float32), near_keys.astype(jnp.float32)) * HEAD_DIM ** (-0.5)
    query_place = jnp.arange(total, dtype=jnp.int32).reshape(blocks, WINDOW)
    key_place = (jnp.arange(blocks, dtype=jnp.int32)[:, None] - 1) * WINDOW + jnp.arange(3 * WINDOW, dtype=jnp.int32)[None, :]
    allowed = (jnp.abs(query_place[:, :, None] - key_place[:, None, :]) <= WINDOW) & (key_place[:, None, :] >= 0) & (key_place[:, None, :] < total)
    scores = jnp.where(allowed[:, None], scores, -1e+30)
    sink_column = sinks[None, :, None]
    top = jnp.maximum(lax.optimization_barrier(jnp.max(scores, axis=-1)), sink_column)
    weights = jnp.exp(scores - top[..., None])
    denominator = lax.optimization_barrier(jnp.sum(weights, axis=-1)) + jnp.exp(sink_column - top)
    shares = (weights / denominator[..., None]).astype(jnp.bfloat16)
    mixed = jnp.einsum('nrqk,nkd->nqrd', shares.astype(jnp.float32), near_values.astype(jnp.float32))
    return mixed.astype(jnp.bfloat16).reshape(total, group * HEAD_DIM)

def mixer_half(mixer_input, mixer_gain, query_weight, key_weight, value_weight, output_weight, sink_logit):
    total = mixer_input.shape[0]
    group = HEADS // KV_HEADS
    normed = normalize(mixer_input, mixer_gain)
    places = jnp.arange(total, dtype=jnp.int32)
    query = jnp.dot(normed, query_weight, preferred_element_type=jnp.float32).reshape(total, HEADS, HEAD_DIM)
    query = axial_rope(query, places).astype(jnp.bfloat16).reshape(total, KV_HEADS, group, HEAD_DIM)
    keys = jnp.dot(normed, key_weight, preferred_element_type=jnp.float32).reshape(total, KV_HEADS, HEAD_DIM)
    keys = axial_rope(keys, places).astype(jnp.bfloat16)
    values = jnp.dot(normed, value_weight, preferred_element_type=jnp.float32).astype(jnp.bfloat16).reshape(total, KV_HEADS, HEAD_DIM)
    mixed = lax.map(band_attention, (query.transpose(1, 0, 2, 3), keys.transpose(1, 0, 2), values.transpose(1, 0, 2), sink_logit.reshape(KV_HEADS, group)))
    mixed = mixed.transpose(1, 0, 2).reshape(total, HEADS * HEAD_DIM)
    return jnp.dot(mixed, output_weight, preferred_element_type=jnp.float32).astype(jnp.bfloat16)

def expert_half(expert_input, expert_gain, routes, route_logits, gate_weight, up_weight, down_weight):
    normed = normalize(expert_input, expert_gain)
    chances = jax.nn.softmax(route_logits, axis=-1)
    chosen = routes.reshape(-1)
    count = chosen.shape[0]
    marks = (chosen[:, None] == jnp.arange(EXPERTS, dtype=jnp.int32)[None, :]).astype(jnp.int32)
    earlier = lax.optimization_barrier(jnp.sum((jnp.cumsum(marks, axis=0) - marks) * marks, axis=1))
    room = N_EP * CAP
    target = chosen * room + earlier
    holder = jnp.full((EXPERTS * room,), count, jnp.int32).at[target].set(jnp.arange(count, dtype=jnp.int32))
    holder = (holder // TOP_K).reshape(EXPERTS, room)
    padded = jnp.concatenate([normed, jnp.zeros((1, normed.shape[1]), jnp.bfloat16)], axis=0)

    def serve(parts):
        token_index, gate_part, up_part, down_part = parts
        rows = padded[token_index]
        gate = jnp.dot(rows, gate_part, preferred_element_type=jnp.float32)
        up = jnp.dot(rows, up_part, preferred_element_type=jnp.float32)
        hidden = activate(gate, up)
        return jnp.dot(hidden, down_part, preferred_element_type=jnp.float32).astype(jnp.bfloat16)
    served = lax.map(serve, (holder, gate_weight, up_weight, down_weight))
    flat = served.reshape(EXPERTS * room, served.shape[2])
    picked = flat[target].astype(jnp.float32).reshape(-1, TOP_K, served.shape[2])
    return lax.optimization_barrier(jnp.sum(picked * chances[:, :, None], axis=1)).astype(jnp.bfloat16)

def reference(mixer_input, mixer_gain, query_weight, key_weight, value_weight, output_weight, sink_logit, expert_input, expert_gain, routes, route_logits, gate_weight, up_weight, down_weight):
    mixer_output = mixer_half(mixer_input, mixer_gain, query_weight, key_weight, value_weight, output_weight, sink_logit)
    expert_output = expert_half(expert_input, expert_gain, routes, route_logits, gate_weight, up_weight, down_weight)
    return (mixer_output, expert_output)
```

```python
import functools

import jax
import jax.numpy as jnp
import numpy as np
from jax import lax
from jax.experimental import pallas as pl
from jax.experimental.pallas import tpu as pltpu
from jax.sharding import PartitionSpec as P

HEAD_DIM = 64
TOP_K = 4
WINDOW = 128
GRID_W = 64


EPSILON = 1e-06
LIMIT = 7.0
SLOPE = 1.702
BASE = 10000.0


def normalize(rows, gain):
    values = rows.astype(jnp.float32)
    scaled = values * lax.rsqrt(jnp.mean(values * values, axis=-1, keepdims=True) + EPSILON)
    return (scaled * gain).astype(jnp.bfloat16)


def rotate(values, cosine, sine):
    width = values.shape[1]
    lanes = cosine.shape[1]
    if width < lanes:
        return rotate(jnp.concatenate([values] * (lanes // width), axis=1), cosine, sine)[:, :width]
    spot = lax.broadcasted_iota(jnp.int32, cosine.shape, 1)
    leading = spot % (HEAD_DIM // 2) < HEAD_DIM // 4
    pieces = []
    for start in range(0, width, lanes):
        piece = values[:, start : start + lanes]
        other = jnp.where(
            leading,
            pltpu.roll(piece, lanes - HEAD_DIM // 4, 1),
            pltpu.roll(piece, HEAD_DIM // 4, 1),
        )
        pieces.append(piece * cosine + other * sine)
    return jnp.concatenate(pieces, axis=1)


def activate(gate, up):
    capped = jnp.minimum(gate, LIMIT)
    bounded = jnp.clip(up, -LIMIT, LIMIT)
    return (capped * jax.nn.sigmoid(SLOPE * capped) * (bounded + 1.0)).astype(jnp.bfloat16)


def remote(src, dst, sent, landed, ep, tp):
    return pltpu.make_async_remote_copy(
        src_ref=src,
        dst_ref=dst,
        send_sem=sent,
        recv_sem=landed,
        device_id=(ep, tp),
        device_id_type=pl.DeviceIdType.MESH,
    )


def exchange(
    n,
    t,
    x_hbm,
    gain_ref,
    logit_ref,
    route_ref,
    mixer_hbm,
    mixer_gain_ref,
    frequency_ref,
    sink_ref,
    wq_hbm,
    wk_hbm,
    wv_hbm,
    wo_hbm,
    wg_hbm,
    wu_hbm,
    wd_hbm,
    mixer_out,
    expert_out,
    x_ref,
    mixer_ref,
    tokens,
    hidden,
    heads,
    shares,
    half_out,
    half_in,
    result,
    returned,
    kept_half,
    queries,
    around,
    wq,
    wk,
    wv,
    wo,
    wg,
    wu,
    wd,
    local_sem,
    token_recv,
    up_send,
    down_send,
    core_send,
    hidden_send,
    hidden_recv,
    pass_send,
    head_send,
    head_recv,
    head_pass_send,
    edge_send,
    edge_recv,
    share_send,
    share_recv,
    half_send,
    half_recv,
    result_send,
    result_recv,
):
    ep, tp = lax.axis_index("ep"), lax.axis_index("tp")
    chips = n // 2
    z, core = ep // 2, ep % 2
    partner = 2 * z + 1 - core
    rows = x_ref.shape[0]
    pair = 2 * rows
    part = wg.shape[1]
    length = mixer_ref.shape[0]
    kept = wk.shape[1]
    spread = wq.shape[1]
    square = t == 4
    direct = (1, 2) if square else tuple(range(1, t))

    def peer(k):
        if not square:
            return lax.rem(tp + k, t)
        return lax.rem(tp + (k // 2) * 2 + (k % 2) * (1 - 2 * (tp % 2)) + t, t)

    def block(index, size):
        return pl.ds(pl.multiple_of(index * size, size), size)

    loads = [
        pltpu.make_async_copy(a, b, local_sem.at[i])
        for i, (a, b) in enumerate((
            (x_hbm, x_ref),
            (wg_hbm, wg),
            (wu_hbm, wu),
            (mixer_hbm, mixer_ref),
            (wk_hbm, wk),
            (wv_hbm, wv),
            (wq_hbm, wq),
            (wd_hbm, wd),
            (wo_hbm, wo),
        ))
    ]
    for load in loads:
        load.start()

    barrier = pltpu.get_barrier_semaphore()
    for k in range(1, n):
        pl.semaphore_signal(
            barrier,
            inc=1,
            device_id=(lax.rem(ep + k, n), tp),
            device_id_type=pl.DeviceIdType.MESH,
        )
    for k in range(1, t):
        pl.semaphore_signal(
            barrier,
            inc=1,
            device_id=(ep, peer(k)),
            device_id_type=pl.DeviceIdType.MESH,
        )

    logits = logit_ref[...]
    raised = jnp.exp(logits - jnp.max(logits, axis=0, keepdims=True))
    chances = raised / jnp.sum(raised, axis=0, keepdims=True)
    number = lax.broadcasted_iota(jnp.int32, (n, rows), 0)
    share = jnp.zeros((n, rows), jnp.float32)
    for k in range(TOP_K):
        share += jnp.where(route_ref[k : k + 1, :] == number, chances[k : k + 1, :], 0.0)
    shares[ep] = share

    loads[0].wait()
    tokens[block(ep, rows), :] = normalize(x_ref[...], gain_ref[...])
    pl.semaphore_wait(barrier, n + t - 2)

    def token_copy(slot, sent, target):
        piece = tokens.at[block(slot, rows)]
        return remote(piece, piece, sent, token_recv.at[slot], target, tp)

    def up_copy(place):
        return token_copy(2 * place + core, up_send.at[place], ep + 2)

    def down_copy(place):
        return token_copy(2 * place + core, down_send.at[place], ep - 2)

    def core_copy(place):
        return token_copy(2 * place + core, core_send.at[place], partner)

    def token_wait(slot):
        token_copy(slot, core_send.at[0], partner).wait_recv()

    def share_copy(k):
        piece = shares.at[ep]
        target = lax.rem(ep + k, n)
        return remote(piece, piece, share_send.at[k], share_recv.at[ep], target, tp)

    def share_wait(slot):
        piece = shares.at[slot]
        remote(piece, piece, share_send.at[0], share_recv.at[slot], partner, tp).wait_recv()

    lowest, highest = z == 0, z == chips - 1

    @pl.when(jnp.logical_not(highest))
    def _():
        up_copy(z).start()

    @pl.when(jnp.logical_not(lowest))
    def _():
        down_copy(z).start()

    core_copy(z).start()
    for k in range(1, n):
        share_copy(k).start()

    def hidden_piece(source, place, half):
        return hidden.at[
            block(2 * place + half, rows), pl.ds(pl.multiple_of(source * part, part), part)
        ]

    def hidden_copy(source, place, half, k):
        piece = hidden_piece(source, place, half)
        return remote(
            piece,
            piece,
            hidden_send.at[k, place, half],
            hidden_recv.at[source, place, half],
            ep,
            peer(k),
        )

    def hidden_forward(place, way):
        source = peer(2 - way)
        piece = hidden_piece(source, place, 1 - way)
        return remote(
            piece,
            piece,
            pass_send.at[way, place],
            hidden_recv.at[source, place, 1 - way],
            ep,
            peer(1 + way),
        )

    def hidden_pass(place):
        if square:
            for way in range(2):
                hidden_copy(peer(2 - way), place, 1 - way, 2 - way).wait_recv()
                hidden_forward(place, way).start()

    def hidden_wait(place):
        for k in range(1, t):
            for half in range(2):
                if not (square and (k, half) in ((1, 0), (2, 1))):
                    hidden_copy(peer(k), place, half, direct[0]).wait_recv()

    def head_piece(source, half):
        return heads.at[
            pl.ds(half * (length // 2), length // 2),
            pl.ds(pl.multiple_of(source * spread, spread), spread),
        ]

    def head_copy(source, half, k):
        piece = head_piece(source, half)
        return remote(
            piece, piece, head_send.at[k, half], head_recv.at[source, half], ep, peer(k)
        )

    def head_forward(way):
        source = peer(2 - way)
        piece = head_piece(source, 1 - way)
        return remote(
            piece,
            piece,
            head_pass_send.at[way],
            head_recv.at[source, 1 - way],
            ep,
            peer(1 + way),
        )

    def head_pass():
        if square:
            for way in range(2):
                head_copy(peer(2 - way), 1 - way, 2 - way).wait_recv()
                head_forward(way).start()

    def head_wait():
        for k in range(1, t):
            for half in range(2):
                if not (square and (k, half) in ((1, 0), (2, 1))):
                    head_copy(peer(k), half, direct[0]).wait_recv()

    def first_half(place):
        token_wait(2 * place + 1 - core)
        inside = block(place, pair)
        span = min(256, part)
        for start in range(0, part, span):
            cut = slice(start, start + span)
            gate = jnp.dot(tokens[inside, :], wg[:, cut], preferred_element_type=jnp.float32)
            up = jnp.dot(tokens[inside, :], wu[:, cut], preferred_element_type=jnp.float32)
            column = pl.ds(pl.multiple_of(tp * part + start, span), span)
            hidden[inside, column] = activate(gate, up)
        for order in range(2):
            for k in direct:
                hidden_copy(tp, place, order if k != 2 else 1 - order, k).start()

    loads[1].wait()
    loads[2].wait()
    first_half(z)

    loads[3].wait()
    normed = normalize(mixer_ref[...], mixer_gain_ref[...])
    lanes = 2 * HEAD_DIM
    spot = lax.broadcasted_iota(jnp.int32, (length, lanes), 1)
    token = ep * length + lax.broadcasted_iota(jnp.int32, (length, lanes), 0)
    turn = jnp.where(spot % HEAD_DIM < HEAD_DIM // 2, token // GRID_W, token % GRID_W)
    turn = turn.astype(jnp.float32) * frequency_ref[...]
    cosine = jnp.cos(turn)
    sine = jnp.sin(turn) * jnp.where(spot % (HEAD_DIM // 2) < HEAD_DIM // 4, -1.0, 1.0)
    own = slice(WINDOW, WINDOW + length)
    for load in loads[4:6]:
        load.wait()
    keys = jnp.dot(normed, wk[...], preferred_element_type=jnp.float32)
    around[own, 0:kept] = rotate(keys, cosine, sine).astype(jnp.bfloat16)
    around[own, kept:] = jnp.dot(normed, wv[...], preferred_element_type=jnp.float32).astype(
        jnp.bfloat16
    )

    def edge_copy(way):
        source, target = (length, 0) if way == 0 else (WINDOW, WINDOW + length)
        return remote(
            around.at[pl.ds(source, WINDOW)],
            around.at[pl.ds(target, WINDOW)],
            edge_send.at[way],
            edge_recv.at[way],
            ep + (1 if way == 0 else -1),
            tp,
        )

    first, last = ep == 0, ep == n - 1

    @pl.when(jnp.logical_not(last))
    def _():
        edge_copy(0).start()

    @pl.when(jnp.logical_not(first))
    def _():
        edge_copy(1).start()

    @pl.when(first)
    def _():
        around[0:WINDOW, :] = jnp.zeros((WINDOW, around.shape[1]), jnp.bfloat16)

    @pl.when(last)
    def _():
        around[WINDOW + length :, :] = jnp.zeros((WINDOW, around.shape[1]), jnp.bfloat16)

    loads[6].wait()
    turned = jnp.dot(normed, wq[...], preferred_element_type=jnp.float32)
    queries[...] = rotate(turned, cosine, sine).astype(jnp.bfloat16)

    def attend(number, carry):
        inside = pl.ds(pl.multiple_of(number * WINDOW, WINDOW), WINDOW)
        seen = pl.ds(pl.multiple_of(number * WINDOW, WINDOW), 3 * WINDOW)
        shape = (WINDOW, 3 * WINDOW)
        line = lax.broadcasted_iota(jnp.int32, shape, 0)
        key = lax.broadcasted_iota(jnp.int32, shape, 1)
        place = ep * length + (number - 1) * WINDOW + key
        allowed = (key >= line) & (key <= line + 2 * WINDOW) & (place >= 0) & (place < n * length)
        group = queries.shape[1] // kept
        allowed = jnp.concatenate([allowed] * group, axis=0)
        for head in range(kept // HEAD_DIM):
            first = head * group
            query = jnp.concatenate(
                [
                    queries[inside, (first + r) * HEAD_DIM : (first + r + 1) * HEAD_DIM]
                    for r in range(group)
                ],
                axis=0,
            )
            sinks = jnp.concatenate(
                [
                    jnp.broadcast_to(sink_ref[:, first + r : first + r + 1], (WINDOW, 1))
                    for r in range(group)
                ],
                axis=0,
            )
            near_keys = around[seen, head * HEAD_DIM : (head + 1) * HEAD_DIM]
            near_values = around[seen, kept + head * HEAD_DIM : kept + (head + 1) * HEAD_DIM]
            scores = lax.dot_general(
                query,
                near_keys,
                (((1,), (1,)), ((), ())),
                preferred_element_type=jnp.float32,
            ) * HEAD_DIM ** (-0.5)
            scores = jnp.where(allowed, scores, -1e30)
            top = jnp.maximum(jnp.max(scores, axis=-1, keepdims=True), sinks)
            weights = jnp.exp(scores - top)
            denominator = jnp.sum(weights, axis=-1, keepdims=True) + jnp.exp(sinks - top)
            share = (weights * (1.0 / denominator)).astype(jnp.bfloat16)
            mixed = jnp.dot(share, near_values, preferred_element_type=jnp.float32)
            mixed = mixed.astype(jnp.bfloat16)
            width = group * HEAD_DIM
            column = pl.ds(pl.multiple_of(tp * spread + first * HEAD_DIM, width), width)
            heads[inside, column] = jnp.concatenate(
                [mixed[r * WINDOW : (r + 1) * WINDOW] for r in range(group)], axis=1
            )
        return carry

    def attention():
        @pl.when(jnp.logical_not(first))
        def _():
            edge_copy(0).wait_recv()

        @pl.when(jnp.logical_not(last))
        def _():
            edge_copy(1).wait_recv()

        lax.fori_loop(0, length // WINDOW, attend, 0)
        for order in range(2):
            for k in direct:
                head_copy(tp, order if k != 2 else 1 - order, k).start()

    def half_copy(place):
        return remote(
            half_out.at[place],
            half_in.at[place],
            half_send.at[place],
            half_recv.at[place],
            partner,
            tp,
        )

    def result_copy(place, source):
        return remote(
            result.at[place],
            returned.at[source],
            result_send.at[place],
            result_recv.at[source],
            2 * place + core,
            tp,
        )

    def scaled(slot):
        total = jnp.dot(hidden[block(slot, rows), :], wd[...], preferred_element_type=jnp.float32)
        line = shares[slot, pl.ds(ep, 1), :]
        column = jnp.transpose(jnp.broadcast_to(line, (rows, rows)))
        return jnp.concatenate(
            [total[:, i : i + rows] * column for i in range(0, total.shape[1], rows)], axis=1
        )

    def second_half(place, mine):
        hidden_wait(place)
        for side in (1 - core, core):
            slot = 2 * place + side
            if mine:
                @pl.when(slot != ep)
                def _():
                    share_wait(slot)
            else:
                share_wait(slot)
        half_out[place] = scaled(2 * place + 1 - core).astype(jnp.bfloat16)
        half_copy(place).start()
        kept_half[...] = scaled(2 * place + core)
        half_copy(place).wait_recv()
        total = kept_half[...] + half_in[place].astype(jnp.float32)
        if mine:
            returned[place] = total.astype(jnp.bfloat16)
        else:
            result[place] = total.astype(jnp.bfloat16)
            result_copy(place, z).start()

    def sides(hop, action):
        def side(k, carry):
            place = z + (2 * k - 1) * hop

            @pl.when((place >= 0) & (place < chips))
            def _():
                action(place, k)

            return carry

        lax.fori_loop(0, 2, side, 0)

    def arrive(hop):
        below, above = z - hop, z + hop

        @pl.when(below >= 0)
        def _():
            token_wait(2 * below + core)

            @pl.when(jnp.logical_not(highest))
            def _():
                up_copy(below).start()

            core_copy(below).start()

        @pl.when(above < chips)
        def _():
            token_wait(2 * above + core)

            @pl.when(jnp.logical_not(lowest))
            def _():
                down_copy(above).start()

            core_copy(above).start()

    def pass_one(hop):
        below, above = z - hop, z + hop

        @pl.when((below >= 0) | (above < chips))
        def _():
            hidden_pass(jnp.where(below >= 0, below, above))

    def pass_two(hop):
        below, above = z - hop, z + hop

        @pl.when((below >= 0) & (above < chips))
        def _():
            hidden_pass(above)

    hidden_pass(z)
    arrive(1)
    sides(1, lambda place, k: first_half(place))
    attention()
    loads[7].wait()
    second_half(z, True)
    pass_one(1)

    def hop_step(hop, carry):
        arrive(hop)
        pass_two(hop - 1)
        sides(hop, lambda place, k: first_half(place))

        @pl.when(hop == 2)
        def _():
            head_pass()

        sides(hop - 1, lambda place, k: second_half(place, False))
        pass_one(hop)
        return carry

    lax.fori_loop(2, chips, hop_step, 0)
    pass_two(chips - 1)
    sides(chips - 1, lambda place, k: second_half(place, False))
    loads[8].wait()
    head_wait()
    mixer_out[...] = jnp.dot(heads[...], wo[...], preferred_element_type=jnp.float32).astype(
        jnp.bfloat16
    )

    for k in range(1, chips):
        source = lax.rem(z + k, chips)
        result_copy(source, source).wait_recv()
    total = returned[0].astype(jnp.float32)
    for source in range(1, chips):
        total += returned[source].astype(jnp.float32)
    expert_out[...] = total.astype(jnp.bfloat16)

    for place in range(chips):
        @pl.when((place <= z) & jnp.logical_not(highest))
        def _():
            up_copy(place).wait_send()

        @pl.when((place >= z) & jnp.logical_not(lowest))
        def _():
            down_copy(place).wait_send()

        core_copy(place).wait_send()
        half_copy(place).wait_send()
        for k in direct:
            for half in range(2):
                hidden_copy(tp, place, half, k).wait_send()
        if square:
            for way in range(2):
                hidden_forward(place, way).wait_send()

        @pl.when(place != z)
        def _():
            result_copy(place, z).wait_send()

    for k in direct:
        for half in range(2):
            head_copy(tp, half, k).wait_send()
    if square:
        for way in range(2):
            head_forward(way).wait_send()

    @pl.when(jnp.logical_not(last))
    def _():
        edge_copy(0).wait_send()

    @pl.when(jnp.logical_not(first))
    def _():
        edge_copy(1).wait_send()

    for k in range(1, n):
        share_copy(k).wait_send()


def shards(
    mixer_input,
    mixer_gain,
    query_weight,
    key_weight,
    value_weight,
    output_weight,
    sink_logit,
    expert_input,
    expert_gain,
    routes,
    route_logits,
    gate_weight,
    up_weight,
    down_weight,
):
    tokens = mixer_input.shape[0]
    lanes = 2 * HEAD_DIM
    quarter = HEAD_DIM // 4
    spot = np.arange(lanes) % quarter
    frequency = (BASE ** (-spot.astype(np.float32) / np.float32(quarter))).astype(np.float32)[None]
    experts = lax.axis_size("ep")
    parts = lax.axis_size("tp")
    rows, width = expert_input.shape
    part = gate_weight.shape[2]
    vmem = pl.BlockSpec(memory_space=pltpu.VMEM)
    anywhere = pl.BlockSpec(memory_space=pl.ANY)
    chips = experts // 2
    dma = pltpu.SemaphoreType.DMA
    columns = down_weight.shape[2]
    spread = query_weight.shape[1]
    half = jnp.bfloat16
    return pl.pallas_call(
        functools.partial(exchange, experts, parts),
        out_shape=(
            jax.ShapeDtypeStruct((tokens, output_weight.shape[1]), half),
            jax.ShapeDtypeStruct((rows, columns), half),
        ),
        in_specs=[anywhere, vmem, vmem, vmem, anywhere, vmem, vmem, vmem] + [anywhere] * 7,
        out_specs=(vmem, vmem),
        scratch_shapes=[
            pltpu.VMEM((rows, width), half),
            pltpu.VMEM(mixer_input.shape, half),
            pltpu.VMEM((experts * rows, width), half),
            pltpu.VMEM((experts * rows, parts * part), half),
            pltpu.VMEM((tokens, parts * spread), half),
            pltpu.VMEM((experts, experts, rows), jnp.float32),
            pltpu.VMEM((chips, rows, columns), half),
            pltpu.VMEM((chips, rows, columns), half),
            pltpu.VMEM((chips, rows, columns), half),
            pltpu.VMEM((chips, rows, columns), half),
            pltpu.VMEM((rows, columns), jnp.float32),
            pltpu.VMEM((tokens, spread), half),
            pltpu.VMEM((tokens + 2 * WINDOW, 2 * key_weight.shape[1]), half),
            pltpu.VMEM(query_weight.shape, half),
            pltpu.VMEM(key_weight.shape, half),
            pltpu.VMEM(value_weight.shape, half),
            pltpu.VMEM(output_weight.shape, half),
            pltpu.VMEM(gate_weight.shape[1:], half),
            pltpu.VMEM(up_weight.shape[1:], half),
            pltpu.VMEM(down_weight.shape[1:], half),
            dma((9,)),
            dma((experts,)),
            dma((chips,)),
            dma((chips,)),
            dma((chips,)),
            dma((parts, chips, 2)),
            dma((parts, chips, 2)),
            dma((2, chips)),
            dma((parts, 2)),
            dma((parts, 2)),
            dma((2,)),
            dma((2,)),
            dma((2,)),
            dma((experts,)),
            dma((experts,)),
            dma((chips,)),
            dma((chips,)),
            dma((chips,)),
            dma((chips,)),
        ],
        compiler_params=pltpu.CompilerParams(
            collective_id=0, has_side_effects=True, vmem_limit_bytes=60 * 1024 * 1024
        ),
    )(
        expert_input,
        expert_gain.reshape(1, -1),
        route_logits.T,
        routes.T,
        mixer_input,
        mixer_gain.reshape(1, -1),
        jnp.asarray(frequency),
        sink_logit.reshape(1, -1),
        query_weight,
        key_weight,
        value_weight,
        output_weight,
        gate_weight[0],
        up_weight[0],
        down_weight[0],
    )


def solution(mesh):
    return jax.shard_map(
        shards,
        mesh=mesh,
        in_specs=(
            P("ep", None),
            P(),
            P(None, "tp"),
            P(None, "tp"),
            P(None, "tp"),
            P(None, "tp"),
            P("tp"),
            P("ep", None),
            P(),
            P("ep", None),
            P("ep", None),
            P("ep", None, "tp"),
            P("ep", None, "tp"),
            P("ep", None, "tp"),
        ),
        out_specs=(P("ep", "tp"), P("ep", "tp")),
        check_vma=False,
    )
```

```python
import functools

import jax
import jax.numpy as jnp
import numpy as np
from jax import lax
from jax.experimental import pallas as pl
from jax.experimental.pallas import tpu as pltpu
from jax.sharding import PartitionSpec as P

HEAD_DIM = 64
TOP_K = 4
WINDOW = 128
GRID_W = 64
SPLIT = 2
EARLY = 0
LATE = 3


EPSILON = 1e-06
LIMIT = 7.0
SLOPE = 1.702
BASE = 10000.0


def normalize(rows, gain):
    values = rows.astype(jnp.float32)
    scaled = values * lax.rsqrt(jnp.mean(values * values, axis=-1, keepdims=True) + EPSILON)
    return (scaled * gain).astype(jnp.bfloat16)


def rotate(values, cosine, sine):
    width = values.shape[1]
    lanes = cosine.shape[1]
    if width < lanes:
        return rotate(jnp.concatenate([values] * (lanes // width), axis=1), cosine, sine)[:, :width]
    spot = lax.broadcasted_iota(jnp.int32, cosine.shape, 1)
    leading = spot % (HEAD_DIM // 2) < HEAD_DIM // 4
    pieces = []
    for start in range(0, width, lanes):
        piece = values[:, start : start + lanes]
        other = jnp.where(
            leading,
            pltpu.roll(piece, lanes - HEAD_DIM // 4, 1),
            pltpu.roll(piece, HEAD_DIM // 4, 1),
        )
        pieces.append(piece * cosine + other * sine)
    return jnp.concatenate(pieces, axis=1)


def activate(gate, up):
    capped = jnp.minimum(gate, LIMIT)
    bounded = jnp.clip(up, -LIMIT, LIMIT)
    return (capped * jax.nn.sigmoid(SLOPE * capped) * (bounded + 1.0)).astype(jnp.bfloat16)


def remote(src, dst, sent, landed, ep, tp):
    return pltpu.make_async_remote_copy(
        src_ref=src,
        dst_ref=dst,
        send_sem=sent,
        recv_sem=landed,
        device_id=(ep, tp),
        device_id_type=pl.DeviceIdType.MESH,
    )


def exchange(
    n,
    t,
    x_hbm,
    gain_ref,
    logit_ref,
    route_ref,
    mixer_hbm,
    mixer_gain_ref,
    frequency_ref,
    sink_ref,
    wq_hbm,
    wk_hbm,
    wv_hbm,
    wo_hbm,
    wg_hbm,
    wu_hbm,
    wd_hbm,
    mixer_out,
    expert_out,
    x_ref,
    mixer_ref,
    tokens,
    hidden,
    heads,
    shares,
    half_out,
    half_in,
    result,
    returned,
    kept_half,
    scales,
    cosine_ref,
    sine_ref,
    queries,
    around,
    wq,
    wk,
    wv,
    wo,
    wg,
    wu,
    wd,
    local_sem,
    token_recv,
    up_send,
    down_send,
    core_send,
    hidden_send,
    hidden_recv,
    pass_send,
    head_send,
    head_recv,
    head_pass_send,
    edge_send,
    edge_recv,
    share_send,
    share_recv,
    half_send,
    half_recv,
    result_send,
    result_recv,
):
    ep, tp = lax.axis_index("ep"), lax.axis_index("tp")
    chips = n // 2
    z, core = ep // 2, ep % 2
    partner = 2 * z + 1 - core
    rows = x_ref.shape[0]
    size = rows // SPLIT
    pair = 2 * size
    part = wg.shape[1]
    length = mixer_ref.shape[0]
    kept = wk.shape[1]
    spread = wq.shape[1]
    square = t == 4
    direct = (1, 2) if square else tuple(range(1, t))

    def peer(k):
        if not square:
            return lax.rem(tp + k, t)
        return lax.rem(tp + (k // 2) * 2 + (k % 2) * (1 - 2 * (tp % 2)) + t, t)

    def block(index, size):
        return pl.ds(pl.multiple_of(index * size, size), size)

    loads = [
        pltpu.make_async_copy(a, b, local_sem.at[i])
        for i, (a, b) in enumerate((
            (x_hbm, x_ref),
            (wg_hbm, wg),
            (wu_hbm, wu),
            (mixer_hbm, mixer_ref),
            (wk_hbm, wk),
            (wv_hbm, wv),
            (wq_hbm, wq),
            (wd_hbm, wd),
            (wo_hbm, wo),
        ))
    ]
    for load in loads:
        load.start()

    barrier = pltpu.get_barrier_semaphore()
    for k in range(1, n):
        pl.semaphore_signal(
            barrier,
            inc=1,
            device_id=(lax.rem(ep + k, n), tp),
            device_id_type=pl.DeviceIdType.MESH,
        )
    for k in range(1, t):
        pl.semaphore_signal(
            barrier,
            inc=1,
            device_id=(ep, peer(k)),
            device_id_type=pl.DeviceIdType.MESH,
        )

    logits = logit_ref[...]
    raised = jnp.exp(logits - jnp.max(logits, axis=0, keepdims=True))
    chances = raised / jnp.sum(raised, axis=0, keepdims=True)
    number = lax.broadcasted_iota(jnp.int32, (n, rows), 0)
    share = jnp.zeros((n, rows), jnp.float32)
    for k in range(TOP_K):
        share += jnp.where(route_ref[k : k + 1, :] == number, chances[k : k + 1, :], 0.0)
    shares[ep] = share

    lanes = 2 * HEAD_DIM
    spot = lax.broadcasted_iota(jnp.int32, (length, lanes), 1)
    token = ep * length + lax.broadcasted_iota(jnp.int32, (length, lanes), 0)
    turn = jnp.where(spot % HEAD_DIM < HEAD_DIM // 2, token // GRID_W, token % GRID_W)
    turn = turn.astype(jnp.float32) * frequency_ref[...]
    cosine_ref[...] = jnp.cos(turn)
    sine_ref[...] = jnp.sin(turn) * jnp.where(spot % (HEAD_DIM // 2) < HEAD_DIM // 4, -1.0, 1.0)

    loads[0].wait()
    fresh = normalize(x_ref[...], gain_ref[...])
    for sub in range(SPLIT):
        inside = block(2 * (z * SPLIT + sub) + core, size)
        tokens[inside, :] = fresh[sub * size : (sub + 1) * size]

    def unit(place, sub):
        return place * SPLIT + sub

    def token_copy(slot, sent, target):
        piece = tokens.at[block(slot, size)]
        return remote(piece, piece, sent, token_recv.at[slot], target, tp)

    def up_copy(place, sub):
        u = unit(place, sub)
        return token_copy(2 * u + core, up_send.at[u], ep + 2)

    def down_copy(place, sub):
        u = unit(place, sub)
        return token_copy(2 * u + core, down_send.at[u], ep - 2)

    def core_copy(place, sub):
        u = unit(place, sub)
        return token_copy(2 * u + core, core_send.at[u], partner)

    def token_wait(slot):
        token_copy(slot, core_send.at[0], partner).wait_recv()

    def share_copy(k):
        piece = shares.at[ep]
        target = lax.rem(ep + k, n)
        return remote(piece, piece, share_send.at[k], share_recv.at[ep], target, tp)

    def share_wait(slot):
        piece = shares.at[slot]
        remote(piece, piece, share_send.at[0], share_recv.at[slot], partner, tp).wait_recv()

    lowest, highest = z == 0, z == chips - 1

    def spread_own(sub):
        @pl.when(jnp.logical_not(highest))
        def _():
            up_copy(z, sub).start()

        @pl.when(jnp.logical_not(lowest))
        def _():
            down_copy(z, sub).start()

    def hidden_piece(source, u, half):
        return hidden.at[
            block(2 * u + half, size), pl.ds(pl.multiple_of(source * part, part), part)
        ]

    def hidden_copy(source, u, half, k):
        piece = hidden_piece(source, u, half)
        return remote(
            piece,
            piece,
            hidden_send.at[k, u, half],
            hidden_recv.at[source, u, half],
            ep,
            peer(k),
        )

    def hidden_forward(u, way):
        source = peer(2 - way)
        piece = hidden_piece(source, u, 1 - way)
        return remote(
            piece,
            piece,
            pass_send.at[way, u],
            hidden_recv.at[source, u, 1 - way],
            ep,
            peer(1 + way),
        )

    def hidden_pass(u):
        if square:
            for way in range(2):
                hidden_copy(peer(2 - way), u, 1 - way, 2 - way).wait_recv()
                hidden_forward(u, way).start()

    def hidden_wait(u):
        for k in range(1, t):
            for half in range(2):
                if not (square and (k, half) in ((1, 0), (2, 1))):
                    hidden_copy(peer(k), u, half, direct[0]).wait_recv()

    def head_piece(source, half):
        return heads.at[
            block(half, length // 2),
            pl.ds(pl.multiple_of(source * spread, spread), spread),
        ]

    def head_copy(source, half, k):
        piece = head_piece(source, half)
        return remote(
            piece, piece, head_send.at[k, half], head_recv.at[source, half], ep, peer(k)
        )

    def head_forward(way):
        source = peer(2 - way)
        piece = head_piece(source, 1 - way)
        return remote(
            piece,
            piece,
            head_pass_send.at[way],
            head_recv.at[source, 1 - way],
            ep,
            peer(1 + way),
        )

    def head_pass():
        if square:
            for way in range(2):
                head_copy(peer(2 - way), 1 - way, 2 - way).wait_recv()
                head_forward(way).start()

    def head_wait():
        for k in range(1, t):
            for half in range(2):
                if not (square and (k, half) in ((1, 0), (2, 1))):
                    head_copy(peer(k), half, direct[0]).wait_recv()

    def expand(slots):
        span = min(256, part)
        for start in range(0, part, span):
            cut = slice(start, start + span)
            lines = jnp.concatenate([tokens[block(slot, size), :] for slot in slots], axis=0)
            gate = jnp.dot(lines, wg[:, cut], preferred_element_type=jnp.float32)
            up = jnp.dot(lines, wu[:, cut], preferred_element_type=jnp.float32)
            column = pl.ds(pl.multiple_of(tp * part + start, span), span)
            active = activate(gate, up)
            for i, slot in enumerate(slots):
                hidden[block(slot, size), column] = active[i * size : (i + 1) * size]

    def first_half(u):
        token_wait(2 * u + 1 - core)
        expand([2 * u, 2 * u + 1])
        for order in range(2):
            for k in direct:
                hidden_copy(tp, u, order if k != 2 else 1 - order, k).start()

    def first_own(side):
        expand([2 * unit(z, sub) + side for sub in range(SPLIT)])

    def send_own(side):
        for sub in range(SPLIT):
            for k in direct:
                hidden_copy(tp, unit(z, sub), side, k).start()

    loads[1].wait()
    loads[2].wait()
    first_own(core)
    pl.semaphore_wait(barrier, n + t - 2)
    for k in range(1, n):
        share_copy(k).start()
    spread_own(0)
    for sub in range(SPLIT):
        core_copy(z, sub).start()
    send_own(core)

    loads[3].wait()
    normed = normalize(mixer_ref[...], mixer_gain_ref[...])
    own = slice(WINDOW, WINDOW + length)
    for load in loads[4:6]:
        load.wait()
    cosine, sine = cosine_ref[...], sine_ref[...]
    keys = jnp.dot(normed, wk[...], preferred_element_type=jnp.float32)
    around[own, 0:kept] = rotate(keys, cosine, sine).astype(jnp.bfloat16)
    around[own, kept:] = jnp.dot(normed, wv[...], preferred_element_type=jnp.float32).astype(
        jnp.bfloat16
    )

    def edge_copy(way):
        source, target = (length, 0) if way == 0 else (WINDOW, WINDOW + length)
        return remote(
            around.at[pl.ds(source, WINDOW)],
            around.at[pl.ds(target, WINDOW)],
            edge_send.at[way],
            edge_recv.at[way],
            ep + (1 if way == 0 else -1),
            tp,
        )

    first, last = ep == 0, ep == n - 1

    @pl.when(jnp.logical_not(last))
    def _():
        edge_copy(0).start()

    @pl.when(jnp.logical_not(first))
    def _():
        edge_copy(1).start()

    for sub in range(1, SPLIT):
        spread_own(sub)

    @pl.when(first)
    def _():
        around[0:WINDOW, :] = jnp.zeros((WINDOW, around.shape[1]), jnp.bfloat16)

    @pl.when(last)
    def _():
        around[WINDOW + length :, :] = jnp.zeros((WINDOW, around.shape[1]), jnp.bfloat16)

    for sub in range(SPLIT):
        token_wait(2 * unit(z, sub) + 1 - core)
    first_own(1 - core)
    send_own(1 - core)

    loads[6].wait()
    turned = jnp.dot(normed, wq[...], preferred_element_type=jnp.float32)
    queries[...] = rotate(turned, cosine, sine).astype(jnp.bfloat16)

    def attend(number, carry):
        inside = pl.ds(pl.multiple_of(number * WINDOW, WINDOW), WINDOW)
        seen = pl.ds(pl.multiple_of(number * WINDOW, WINDOW), 3 * WINDOW)
        shape = (WINDOW, 3 * WINDOW)
        line = lax.broadcasted_iota(jnp.int32, shape, 0)
        key = lax.broadcasted_iota(jnp.int32, shape, 1)
        place = ep * length + (number - 1) * WINDOW + key
        allowed = (key >= line) & (key <= line + 2 * WINDOW) & (place >= 0) & (place < n * length)
        group = queries.shape[1] // kept
        allowed = jnp.concatenate([allowed] * group, axis=0)
        for head in range(kept // HEAD_DIM):
            first = head * group
            query = jnp.concatenate(
                [
                    queries[inside, (first + r) * HEAD_DIM : (first + r + 1) * HEAD_DIM]
                    for r in range(group)
                ],
                axis=0,
            )
            sinks = jnp.concatenate(
                [
                    jnp.broadcast_to(sink_ref[:, first + r : first + r + 1], (WINDOW, 1))
                    for r in range(group)
                ],
                axis=0,
            )
            near_keys = around[seen, head * HEAD_DIM : (head + 1) * HEAD_DIM]
            near_values = around[seen, kept + head * HEAD_DIM : kept + (head + 1) * HEAD_DIM]
            scores = lax.dot_general(
                query,
                near_keys,
                (((1,), (1,)), ((), ())),
                preferred_element_type=jnp.float32,
            ) * HEAD_DIM ** (-0.5)
            scores = jnp.where(allowed, scores, -1e30)
            top = jnp.maximum(jnp.max(scores, axis=-1, keepdims=True), sinks)
            weights = jnp.exp(scores - top)
            denominator = jnp.sum(weights, axis=-1, keepdims=True) + jnp.exp(sinks - top)
            share = (weights * (1.0 / denominator)).astype(jnp.bfloat16)
            mixed = jnp.dot(share, near_values, preferred_element_type=jnp.float32)
            mixed = mixed.astype(jnp.bfloat16)
            width = group * HEAD_DIM
            column = pl.ds(pl.multiple_of(tp * spread + first * HEAD_DIM, width), width)
            heads[inside, column] = jnp.concatenate(
                [mixed[r * WINDOW : (r + 1) * WINDOW] for r in range(group)], axis=1
            )
        return carry

    def attention(half):
        @pl.when((half == 0) & jnp.logical_not(first))
        def _():
            edge_copy(0).wait_recv()

        @pl.when((half == 1) & jnp.logical_not(last))
        def _():
            edge_copy(1).wait_recv()

        count = length // 2 // WINDOW
        lax.fori_loop(half * count, (half + 1) * count, attend, 0)
        for k in direct:
            head_copy(tp, half, k).start()

    def half_copy(u):
        return remote(
            half_out.at[u], half_in.at[u], half_send.at[u], half_recv.at[u], partner, tp
        )

    def result_copy(u, source):
        return remote(
            result.at[u],
            returned.at[source, u % SPLIT],
            result_send.at[u],
            result_recv.at[source, u % SPLIT],
            2 * (u // SPLIT) + core,
            tp,
        )

    def spread_shares(slot, carry):
        @pl.when(slot != ep)
        def _():
            share_wait(slot)

        line = shares[slot, pl.ds(ep, 1), :]
        column = jnp.transpose(jnp.broadcast_to(line, (rows, rows)))
        for sub in range(SPLIT):
            inside = block(2 * unit(slot // 2, sub) + slot % 2, size)
            scales[inside, :] = column[sub * size : (sub + 1) * size]
        return carry

    def scaled(slot):
        inside = block(slot, size)
        total = jnp.dot(hidden[inside, :], wd[...], preferred_element_type=jnp.float32)
        column = scales[inside, :]
        return jnp.concatenate(
            [total[:, i : i + rows] * column for i in range(0, total.shape[1], rows)], axis=1
        )

    def second_half(u):
        hidden_wait(u)
        half_out[u] = scaled(2 * u + 1 - core).astype(jnp.bfloat16)
        half_copy(u).start()
        kept_half[u] = scaled(2 * u + core)

    def combine(u):
        half_copy(u).wait_recv()
        total = kept_half[u] + half_in[u].astype(jnp.float32)
        result[u] = total.astype(jnp.bfloat16)

    def sides(hop, action):
        def side(k, carry):
            place = z + (2 * k - 1) * hop

            @pl.when((place >= 0) & (place < chips))
            def _():
                action(place, k)

            return carry

        lax.fori_loop(0, 2, side, 0)

    def arrive(hop, sub):
        below, above = z - hop, z + hop

        @pl.when(below >= 0)
        def _():
            token_wait(2 * unit(below, sub) + core)

            @pl.when(jnp.logical_not(highest))
            def _():
                up_copy(below, sub).start()

            core_copy(below, sub).start()

        @pl.when(above < chips)
        def _():
            token_wait(2 * unit(above, sub) + core)

            @pl.when(jnp.logical_not(lowest))
            def _():
                down_copy(above, sub).start()

            core_copy(above, sub).start()

    steps = (chips - 1) * SPLIT

    def one(index, action):
        hop, sub = 1 + index // SPLIT, index % SPLIT
        below, above = z - hop, z + hop

        @pl.when((below >= 0) | (above < chips))
        def _():
            action(unit(jnp.where(below >= 0, below, above), sub))

    def two(index, action):
        hop, sub = 1 + index // SPLIT, index % SPLIT
        below, above = z - hop, z + hop

        @pl.when((below >= 0) & (above < chips))
        def _():
            action(unit(above, sub))

    def deliver(u):
        combine(u)
        result_copy(u, z).start()

    ending = lowest | highest
    look = jnp.where(ending, EARLY, LATE)

    def own_units(action):
        for sub in range(SPLIT):
            action(unit(z, sub))

    def project():
        head_wait()
        mixer_out[...] = jnp.dot(heads[...], wo[...], preferred_element_type=jnp.float32).astype(
            jnp.bfloat16
        )

    def drain(u, carry):
        place, sub = u // SPLIT, u % SPLIT

        @pl.when((place <= z) & jnp.logical_not(highest))
        def _():
            up_copy(place, sub).wait_send()

        @pl.when((place >= z) & jnp.logical_not(lowest))
        def _():
            down_copy(place, sub).wait_send()

        core_copy(place, sub).wait_send()
        half_copy(u).wait_send()
        for k in direct:
            for half in range(2):
                hidden_copy(tp, u, half, k).wait_send()
        if square:
            for way in range(2):
                hidden_forward(u, way).wait_send()

        @pl.when(place != z)
        def _():
            result_copy(u, z).wait_send()

        return carry

    units = chips * SPLIT

    def step(index, carry):
        hop, sub = 1 + index // SPLIT, index % SPLIT
        arrive(hop, sub)
        sides(hop, lambda place, k: first_half(unit(place, sub)))

        @pl.when(index == 0)
        def _():
            for own_sub in range(1, SPLIT):
                hidden_pass(unit(z, own_sub))

        @pl.when(index > 0)
        def _():
            one(index - 1, hidden_pass)

        @pl.when(index > 1)
        def _():
            two(index - 2, hidden_pass)

        @pl.when((index >= look) & (index < look + 2))
        def _():
            attention(index - look)

        @pl.when((index == 3) & ending)
        def _():
            head_pass()

        @pl.when(index > 2)
        def _():
            one(index - 3, deliver)

        @pl.when(index > 1)
        def _():
            one(index - 2, second_half)

        @pl.when(index > 3)
        def _():
            two(index - 4, deliver)

        @pl.when(index > 2)
        def _():
            two(index - 3, second_half)

        return carry

    loads[7].wait()
    lax.fori_loop(0, n, spread_shares, 0)
    hidden_pass(unit(z, 0))
    lax.fori_loop(0, steps, step, 0)
    loads[8].wait()
    second_half(unit(z, 0))
    one(steps - 1, hidden_pass)
    two(steps - 2, hidden_pass)
    two(steps - 1, hidden_pass)
    one(steps - 3, deliver)
    two(steps - 4, deliver)
    for sub in range(1, SPLIT):
        second_half(unit(z, sub))
    one(steps - 2, second_half)
    two(steps - 3, second_half)

    @pl.when(ending)
    def _():
        project()

    two(steps - 3, deliver)
    one(steps - 2, deliver)
    one(steps - 1, second_half)
    two(steps - 2, second_half)
    two(steps - 1, second_half)
    one(steps - 1, deliver)
    two(steps - 2, deliver)
    two(steps - 1, deliver)

    @pl.when(jnp.logical_not(ending))
    def _():
        head_pass()
        project()

    own_units(combine)
    lax.fori_loop(0, units, drain, 0)

    for sub in range(SPLIT):
        total = result[unit(z, sub)].astype(jnp.float32)
        for k in range(1, chips):
            source = lax.rem(z + k, chips)
            result_copy(unit(source, sub), source).wait_recv()
            total += returned[source, sub].astype(jnp.float32)
        expert_out[sub * size : (sub + 1) * size, :] = total.astype(jnp.bfloat16)


    for k in direct:
        for half in range(2):
            head_copy(tp, half, k).wait_send()
    if square:
        for way in range(2):
            head_forward(way).wait_send()

    @pl.when(jnp.logical_not(last))
    def _():
        edge_copy(0).wait_send()

    @pl.when(jnp.logical_not(first))
    def _():
        edge_copy(1).wait_send()

    for k in range(1, n):
        share_copy(k).wait_send()


def shards(
    mixer_input,
    mixer_gain,
    query_weight,
    key_weight,
    value_weight,
    output_weight,
    sink_logit,
    expert_input,
    expert_gain,
    routes,
    route_logits,
    gate_weight,
    up_weight,
    down_weight,
):
    tokens = mixer_input.shape[0]
    lanes = 2 * HEAD_DIM
    quarter = HEAD_DIM // 4
    spot = np.arange(lanes) % quarter
    frequency = (BASE ** (-spot.astype(np.float32) / np.float32(quarter))).astype(np.float32)[None]
    experts = lax.axis_size("ep")
    parts = lax.axis_size("tp")
    rows, width = expert_input.shape
    part = gate_weight.shape[2]
    vmem = pl.BlockSpec(memory_space=pltpu.VMEM)
    anywhere = pl.BlockSpec(memory_space=pl.ANY)
    chips = experts // 2
    dma = pltpu.SemaphoreType.DMA
    columns = down_weight.shape[2]
    spread = query_weight.shape[1]
    half = jnp.bfloat16
    size, units = rows // SPLIT, chips * SPLIT
    return pl.pallas_call(
        functools.partial(exchange, experts, parts),
        out_shape=(
            jax.ShapeDtypeStruct((tokens, output_weight.shape[1]), half),
            jax.ShapeDtypeStruct((rows, columns), half),
        ),
        in_specs=[anywhere, vmem, vmem, vmem, anywhere, vmem, vmem, vmem] + [anywhere] * 7,
        out_specs=(vmem, vmem),
        scratch_shapes=[
            pltpu.VMEM((rows, width), half),
            pltpu.VMEM(mixer_input.shape, half),
            pltpu.VMEM((experts * rows, width), half),
            pltpu.VMEM((experts * rows, parts * part), half),
            pltpu.VMEM((tokens, parts * spread), half),
            pltpu.VMEM((experts, experts, rows), jnp.float32),
            pltpu.VMEM((units, size, columns), half),
            pltpu.VMEM((units, size, columns), half),
            pltpu.VMEM((units, size, columns), half),
            pltpu.VMEM((chips, SPLIT, size, columns), half),
            pltpu.VMEM((units, size, columns), jnp.float32),
            pltpu.VMEM((experts * rows, rows), jnp.float32),
            pltpu.VMEM((tokens, lanes), jnp.float32),
            pltpu.VMEM((tokens, lanes), jnp.float32),
            pltpu.VMEM((tokens, spread), half),
            pltpu.VMEM((tokens + 2 * WINDOW, 2 * key_weight.shape[1]), half),
            pltpu.VMEM(query_weight.shape, half),
            pltpu.VMEM(key_weight.shape, half),
            pltpu.VMEM(value_weight.shape, half),
            pltpu.VMEM(output_weight.shape, half),
            pltpu.VMEM(gate_weight.shape[1:], half),
            pltpu.VMEM(up_weight.shape[1:], half),
            pltpu.VMEM(down_weight.shape[1:], half),
            dma((9,)),
            dma((2 * units,)),
            dma((units,)),
            dma((units,)),
            dma((units,)),
            dma((parts, units, 2)),
            dma((parts, units, 2)),
            dma((2, units)),
            dma((parts, 2)),
            dma((parts, 2)),
            dma((2,)),
            dma((2,)),
            dma((2,)),
            dma((experts,)),
            dma((experts,)),
            dma((units,)),
            dma((units,)),
            dma((units,)),
            dma((chips, SPLIT)),
        ],
        compiler_params=pltpu.CompilerParams(
            collective_id=0, has_side_effects=True, vmem_limit_bytes=60 * 1024 * 1024
        ),
    )(
        expert_input,
        expert_gain.reshape(1, -1),
        route_logits.T,
        routes.T,
        mixer_input,
        mixer_gain.reshape(1, -1),
        jnp.asarray(frequency),
        sink_logit.reshape(1, -1),
        query_weight,
        key_weight,
        value_weight,
        output_weight,
        gate_weight[0],
        up_weight[0],
        down_weight[0],
    )


def solution(mesh):
    return jax.shard_map(
        shards,
        mesh=mesh,
        in_specs=(
            P("ep", None),
            P(),
            P(None, "tp"),
            P(None, "tp"),
            P(None, "tp"),
            P(None, "tp"),
            P("tp"),
            P("ep", None),
            P(),
            P("ep", None),
            P("ep", None),
            P("ep", None, "tp"),
            P("ep", None, "tp"),
            P("ep", None, "tp"),
        ),
        out_specs=(P("ep", "tp"), P("ep", "tp")),
        check_vma=False,
    )
```

```python
import functools

import jax
import jax.numpy as jnp
import numpy as np
from jax import lax
from jax.experimental import pallas as pl
from jax.experimental.pallas import tpu as pltpu
from jax.sharding import PartitionSpec as P

HEAD_DIM = 64
TOP_K = 4
WINDOW = 128
GRID_W = 64
SPLIT = 2
EARLY = 0
LATE = 3


EPSILON = 1e-06
LIMIT = 7.0
SLOPE = 1.702
BASE = 10000.0


def normalize(rows, gain):
    values = rows.astype(jnp.float32)
    scaled = values * lax.rsqrt(jnp.mean(values * values, axis=-1, keepdims=True) + EPSILON)
    return (scaled * gain).astype(jnp.bfloat16)


def rotate(values, cosine, sine):
    width = values.shape[1]
    lanes = cosine.shape[1]
    if width < lanes:
        return rotate(jnp.concatenate([values] * (lanes // width), axis=1), cosine, sine)[:, :width]
    spot = lax.broadcasted_iota(jnp.int32, cosine.shape, 1)
    leading = spot % (HEAD_DIM // 2) < HEAD_DIM // 4
    pieces = []
    for start in range(0, width, lanes):
        piece = values[:, start : start + lanes]
        other = jnp.where(
            leading,
            pltpu.roll(piece, lanes - HEAD_DIM // 4, 1),
            pltpu.roll(piece, HEAD_DIM // 4, 1),
        )
        pieces.append(piece * cosine + other * sine)
    return jnp.concatenate(pieces, axis=1)


def activate(gate, up):
    capped = jnp.minimum(gate, LIMIT)
    bounded = jnp.clip(up, -LIMIT, LIMIT)
    return (capped * jax.nn.sigmoid(SLOPE * capped) * (bounded + 1.0)).astype(jnp.bfloat16)


def remote(src, dst, sent, landed, ep, tp):
    return pltpu.make_async_remote_copy(
        src_ref=src,
        dst_ref=dst,
        send_sem=sent,
        recv_sem=landed,
        device_id=(ep, tp),
        device_id_type=pl.DeviceIdType.MESH,
    )


def exchange(
    n,
    t,
    x_hbm,
    gain_hbm,
    logit_hbm,
    route_hbm,
    mixer_hbm,
    mixer_gain_hbm,
    frequency_hbm,
    sink_hbm,
    wq_hbm,
    wk_hbm,
    wv_hbm,
    wo_hbm,
    wg_hbm,
    wu_hbm,
    wd_hbm,
    mixer_out,
    expert_out,
    gain_ref,
    logit_ref,
    route_ref,
    mixer_gain_ref,
    frequency_ref,
    sink_ref,
    x_ref,
    mixer_ref,
    tokens,
    hidden,
    heads,
    shares,
    half_out,
    half_in,
    result,
    returned,
    kept_half,
    scales,
    cosine_ref,
    sine_ref,
    queries,
    around,
    wq,
    wk,
    wv,
    wo,
    wg,
    wu,
    wd,
    local_sem,
    token_recv,
    up_send,
    down_send,
    core_send,
    hidden_send,
    hidden_recv,
    pass_send,
    head_send,
    head_recv,
    head_pass_send,
    edge_send,
    edge_recv,
    share_send,
    share_recv,
    half_send,
    half_recv,
    result_send,
    result_recv,
):
    ep, tp = lax.axis_index("ep"), lax.axis_index("tp")
    chips = n // 2
    z, core = ep // 2, ep % 2
    partner = 2 * z + 1 - core
    rows = x_ref.shape[0]
    size = rows // SPLIT
    pair = 2 * size
    part = wg.shape[1]
    length = mixer_ref.shape[0]
    kept = wk.shape[1]
    spread = wq.shape[1]
    square = t == 4
    direct = (1, 2) if square else tuple(range(1, t))

    def peer(k):
        if not square:
            return lax.rem(tp + k, t)
        return lax.rem(tp + (k // 2) * 2 + (k % 2) * (1 - 2 * (tp % 2)) + t, t)

    def block(index, size):
        return pl.ds(pl.multiple_of(index * size, size), size)

    loads = [
        pltpu.make_async_copy(a, b, local_sem.at[i])
        for i, (a, b) in enumerate((
            (x_hbm, x_ref),
            (wg_hbm, wg),
            (wu_hbm, wu),
            (mixer_hbm, mixer_ref),
            (wk_hbm, wk),
            (wv_hbm, wv),
            (wq_hbm, wq),
            (wd_hbm, wd),
            (wo_hbm, wo),
            (frequency_hbm, frequency_ref),
            (logit_hbm, logit_ref),
            (route_hbm, route_ref),
            (gain_hbm, gain_ref),
            (mixer_gain_hbm, mixer_gain_ref),
            (sink_hbm, sink_ref),
        ))
    ]
    for load in loads[9:] + loads[:9]:
        load.start()

    barrier = pltpu.get_barrier_semaphore()
    for k in range(1, n):
        pl.semaphore_signal(
            barrier,
            inc=1,
            device_id=(lax.rem(ep + k, n), tp),
            device_id_type=pl.DeviceIdType.MESH,
        )
    for k in range(1, t):
        pl.semaphore_signal(
            barrier,
            inc=1,
            device_id=(ep, peer(k)),
            device_id_type=pl.DeviceIdType.MESH,
        )

    for load in loads[9:]:
        load.wait()
    logits = logit_ref[...]
    raised = jnp.exp(logits - jnp.max(logits, axis=0, keepdims=True))
    chances = raised / jnp.sum(raised, axis=0, keepdims=True)
    number = lax.broadcasted_iota(jnp.int32, (n, rows), 0)
    share = jnp.zeros((n, rows), jnp.float32)
    for k in range(TOP_K):
        share += jnp.where(route_ref[k : k + 1, :] == number, chances[k : k + 1, :], 0.0)
    shares[ep] = share

    lanes = 2 * HEAD_DIM
    spot = lax.broadcasted_iota(jnp.int32, (length, lanes), 1)
    token = ep * length + lax.broadcasted_iota(jnp.int32, (length, lanes), 0)
    turn = jnp.where(spot % HEAD_DIM < HEAD_DIM // 2, token // GRID_W, token % GRID_W)
    turn = turn.astype(jnp.float32) * frequency_ref[...]
    cosine_ref[...] = jnp.cos(turn)
    sine_ref[...] = jnp.sin(turn) * jnp.where(spot % (HEAD_DIM // 2) < HEAD_DIM // 4, -1.0, 1.0)

    loads[0].wait()
    fresh = normalize(x_ref[...], gain_ref[...])
    for sub in range(SPLIT):
        inside = block(2 * (z * SPLIT + sub) + core, size)
        tokens[inside, :] = fresh[sub * size : (sub + 1) * size]

    def unit(place, sub):
        return place * SPLIT + sub

    def token_copy(slot, sent, target):
        piece = tokens.at[block(slot, size)]
        return remote(piece, piece, sent, token_recv.at[slot], target, tp)

    def up_copy(place, sub):
        u = unit(place, sub)
        return token_copy(2 * u + core, up_send.at[u], ep + 2)

    def down_copy(place, sub):
        u = unit(place, sub)
        return token_copy(2 * u + core, down_send.at[u], ep - 2)

    def core_copy(place, sub):
        u = unit(place, sub)
        return token_copy(2 * u + core, core_send.at[0], partner)

    def token_wait(slot):
        token_copy(slot, core_send.at[0], partner).wait_recv()

    def share_copy(k):
        piece = shares.at[ep]
        target = lax.rem(ep + k, n)
        return remote(piece, piece, share_send.at[0], share_recv.at[ep], target, tp)

    def share_wait(slot):
        piece = shares.at[slot]
        remote(piece, piece, share_send.at[0], share_recv.at[slot], partner, tp).wait_recv()

    lowest, highest = z == 0, z == chips - 1

    def spread_own(sub):
        @pl.when(jnp.logical_not(highest))
        def _():
            up_copy(z, sub).start()

        @pl.when(jnp.logical_not(lowest))
        def _():
            down_copy(z, sub).start()

    def hidden_piece(source, u, half):
        return hidden.at[
            block(2 * u + half, size), pl.ds(pl.multiple_of(source * part, part), part)
        ]

    def hidden_copy(source, u, half, k):
        piece = hidden_piece(source, u, half)
        return remote(
            piece,
            piece,
            hidden_send.at[k],
            hidden_recv.at[source, u, half],
            ep,
            peer(k),
        )

    def hidden_forward(u, way):
        source = peer(2 - way)
        piece = hidden_piece(source, u, 1 - way)
        return remote(
            piece,
            piece,
            pass_send.at[way],
            hidden_recv.at[source, u, 1 - way],
            ep,
            peer(1 + way),
        )

    def hidden_pass(u):
        if square:
            for way in range(2):
                hidden_copy(peer(2 - way), u, 1 - way, 2 - way).wait_recv()
                hidden_forward(u, way).start()

    def hidden_wait(u):
        for k in range(1, t):
            for half in range(2):
                if not (square and (k, half) in ((1, 0), (2, 1))):
                    hidden_copy(peer(k), u, half, direct[0]).wait_recv()

    def head_piece(source, half):
        return heads.at[
            block(half, length // 2),
            pl.ds(pl.multiple_of(source * spread, spread), spread),
        ]

    def head_copy(source, half, k):
        piece = head_piece(source, half)
        return remote(
            piece, piece, head_send.at[k], head_recv.at[source, half], ep, peer(k)
        )

    def head_forward(way):
        source = peer(2 - way)
        piece = head_piece(source, 1 - way)
        return remote(
            piece,
            piece,
            head_pass_send.at[way],
            head_recv.at[source, 1 - way],
            ep,
            peer(1 + way),
        )

    def head_pass():
        if square:
            for way in range(2):
                head_copy(peer(2 - way), 1 - way, 2 - way).wait_recv()
                head_forward(way).start()

    def head_wait():
        for k in range(1, t):
            for half in range(2):
                if not (square and (k, half) in ((1, 0), (2, 1))):
                    head_copy(peer(k), half, direct[0]).wait_recv()

    def expand(slots):
        span = min(256, part)
        for start in range(0, part, span):
            cut = slice(start, start + span)
            lines = jnp.concatenate([tokens[block(slot, size), :] for slot in slots], axis=0)
            gate = jnp.dot(lines, wg[:, cut], preferred_element_type=jnp.float32)
            up = jnp.dot(lines, wu[:, cut], preferred_element_type=jnp.float32)
            column = pl.ds(pl.multiple_of(tp * part + start, span), span)
            active = activate(gate, up)
            for i, slot in enumerate(slots):
                hidden[block(slot, size), column] = active[i * size : (i + 1) * size]

    def first_half(u):
        token_wait(2 * u + 1 - core)
        expand([2 * u, 2 * u + 1])
        for order in range(2):
            for k in direct:
                hidden_copy(tp, u, order if k != 2 else 1 - order, k).start()

    def first_own(side):
        expand([2 * unit(z, sub) + side for sub in range(SPLIT)])

    def send_own(side):
        for sub in range(SPLIT):
            for k in direct:
                hidden_copy(tp, unit(z, sub), side, k).start()

    pl.semaphore_wait(barrier, n + t - 2)
    for k in range(1, n):
        share_copy(k).start()
    spread_own(0)
    for sub in range(SPLIT):
        core_copy(z, sub).start()
    loads[1].wait()
    loads[2].wait()
    first_own(core)
    send_own(core)

    loads[3].wait()
    normed = normalize(mixer_ref[...], mixer_gain_ref[...])
    own = slice(WINDOW, WINDOW + length)
    for load in loads[4:6]:
        load.wait()
    cosine, sine = cosine_ref[...], sine_ref[...]
    keys = jnp.dot(normed, wk[...], preferred_element_type=jnp.float32)
    around[own, 0:kept] = rotate(keys, cosine, sine).astype(jnp.bfloat16)
    around[own, kept:] = jnp.dot(normed, wv[...], preferred_element_type=jnp.float32).astype(
        jnp.bfloat16
    )

    def edge_copy(way):
        source, target = (length, 0) if way == 0 else (WINDOW, WINDOW + length)
        return remote(
            around.at[pl.ds(source, WINDOW)],
            around.at[pl.ds(target, WINDOW)],
            edge_send.at[way],
            edge_recv.at[way],
            ep + (1 if way == 0 else -1),
            tp,
        )

    first, last = ep == 0, ep == n - 1

    @pl.when(jnp.logical_not(last))
    def _():
        edge_copy(0).start()

    @pl.when(jnp.logical_not(first))
    def _():
        edge_copy(1).start()

    for sub in range(1, SPLIT):
        spread_own(sub)

    @pl.when(first)
    def _():
        around[0:WINDOW, :] = jnp.zeros((WINDOW, around.shape[1]), jnp.bfloat16)

    @pl.when(last)
    def _():
        around[WINDOW + length :, :] = jnp.zeros((WINDOW, around.shape[1]), jnp.bfloat16)

    for sub in range(SPLIT):
        token_wait(2 * unit(z, sub) + 1 - core)
    first_own(1 - core)
    send_own(1 - core)

    loads[6].wait()
    turned = jnp.dot(normed, wq[...], preferred_element_type=jnp.float32)
    queries[...] = rotate(turned, cosine, sine).astype(jnp.bfloat16)

    def attend(number, carry):
        inside = pl.ds(pl.multiple_of(number * WINDOW, WINDOW), WINDOW)
        seen = pl.ds(pl.multiple_of(number * WINDOW, WINDOW), 3 * WINDOW)
        shape = (WINDOW, 3 * WINDOW)
        line = lax.broadcasted_iota(jnp.int32, shape, 0)
        key = lax.broadcasted_iota(jnp.int32, shape, 1)
        place = ep * length + (number - 1) * WINDOW + key
        allowed = (key >= line) & (key <= line + 2 * WINDOW) & (place >= 0) & (place < n * length)
        group = queries.shape[1] // kept
        allowed = jnp.concatenate([allowed] * group, axis=0)
        for head in range(kept // HEAD_DIM):
            first = head * group
            query = jnp.concatenate(
                [
                    queries[inside, (first + r) * HEAD_DIM : (first + r + 1) * HEAD_DIM]
                    for r in range(group)
                ],
                axis=0,
            )
            sinks = jnp.concatenate(
                [
                    jnp.broadcast_to(sink_ref[:, first + r : first + r + 1], (WINDOW, 1))
                    for r in range(group)
                ],
                axis=0,
            )
            near_keys = around[seen, head * HEAD_DIM : (head + 1) * HEAD_DIM]
            near_values = around[seen, kept + head * HEAD_DIM : kept + (head + 1) * HEAD_DIM]
            scores = lax.dot_general(
                query,
                near_keys,
                (((1,), (1,)), ((), ())),
                preferred_element_type=jnp.float32,
            ) * HEAD_DIM ** (-0.5)
            scores = jnp.where(allowed, scores, -1e30)
            top = jnp.maximum(jnp.max(scores, axis=-1, keepdims=True), sinks)
            weights = jnp.exp(scores - top)
            denominator = jnp.sum(weights, axis=-1, keepdims=True) + jnp.exp(sinks - top)
            share = (weights * (1.0 / denominator)).astype(jnp.bfloat16)
            mixed = jnp.dot(share, near_values, preferred_element_type=jnp.float32)
            mixed = mixed.astype(jnp.bfloat16)
            width = group * HEAD_DIM
            column = pl.ds(pl.multiple_of(tp * spread + first * HEAD_DIM, width), width)
            heads[inside, column] = jnp.concatenate(
                [mixed[r * WINDOW : (r + 1) * WINDOW] for r in range(group)], axis=1
            )
        return carry

    def attention(half):
        @pl.when((half == 0) & jnp.logical_not(first))
        def _():
            edge_copy(0).wait_recv()

        @pl.when((half == 1) & jnp.logical_not(last))
        def _():
            edge_copy(1).wait_recv()

        count = length // 2 // WINDOW
        lax.fori_loop(half * count, (half + 1) * count, attend, 0)
        for k in direct:
            head_copy(tp, half, k).start()

    def half_copy(u):
        return remote(
            half_out.at[u], half_in.at[u], half_send.at[0], half_recv.at[u], partner, tp
        )

    def result_copy(u, source):
        return remote(
            result.at[u],
            returned.at[source, u % SPLIT],
            result_send.at[0],
            result_recv.at[source, u % SPLIT],
            2 * (u // SPLIT) + core,
            tp,
        )

    def spread_shares(slot, carry):
        @pl.when(slot != ep)
        def _():
            share_wait(slot)

        line = shares[slot, pl.ds(ep, 1), :]
        column = jnp.transpose(jnp.broadcast_to(line, (rows, rows)))
        for sub in range(SPLIT):
            inside = block(2 * unit(slot // 2, sub) + slot % 2, size)
            scales[inside, :] = column[sub * size : (sub + 1) * size]
        return carry

    def second_half(u):
        hidden_wait(u)
        inside = block(u, pair)
        total = jnp.dot(hidden[inside, :], wd[...], preferred_element_type=jnp.float32)
        column = scales[inside, :]
        kept_half[u] = jnp.concatenate(
            [total[:, i : i + rows] * column for i in range(0, total.shape[1], rows)], axis=1
        )
        half_out[u] = kept_half[u, block(1 - core, size), :].astype(jnp.bfloat16)
        half_copy(u).start()

    def combine(u):
        half_copy(u).wait_recv()
        total = kept_half[u, block(core, size), :] + half_in[u].astype(jnp.float32)
        result[u] = total.astype(jnp.bfloat16)

    def sides(hop, action):
        def side(k, carry):
            place = z + (2 * k - 1) * hop

            @pl.when((place >= 0) & (place < chips))
            def _():
                action(place, k)

            return carry

        lax.fori_loop(0, 2, side, 0)

    def arrive(hop, sub):
        below, above = z - hop, z + hop

        @pl.when(below >= 0)
        def _():
            token_wait(2 * unit(below, sub) + core)

            @pl.when(jnp.logical_not(highest))
            def _():
                up_copy(below, sub).start()

            core_copy(below, sub).start()

        @pl.when(above < chips)
        def _():
            token_wait(2 * unit(above, sub) + core)

            @pl.when(jnp.logical_not(lowest))
            def _():
                down_copy(above, sub).start()

            core_copy(above, sub).start()

    steps = (chips - 1) * SPLIT

    def one(index, action):
        hop, sub = 1 + index // SPLIT, index % SPLIT
        below, above = z - hop, z + hop

        @pl.when((below >= 0) | (above < chips))
        def _():
            action(unit(jnp.where(below >= 0, below, above), sub))

    def two(index, action):
        hop, sub = 1 + index // SPLIT, index % SPLIT
        below, above = z - hop, z + hop

        @pl.when((below >= 0) & (above < chips))
        def _():
            action(unit(above, sub))

    def deliver(u):
        combine(u)
        result_copy(u, z).start()

    ending = lowest | highest
    look = jnp.where(ending, EARLY, LATE)

    def own_units(action):
        for sub in range(SPLIT):
            action(unit(z, sub))

    def project():
        head_wait()
        mixer_out[...] = jnp.dot(heads[...], wo[...], preferred_element_type=jnp.float32).astype(
            jnp.bfloat16
        )

    def drain(u, carry):
        place, sub = u // SPLIT, u % SPLIT

        @pl.when((place <= z) & jnp.logical_not(highest))
        def _():
            up_copy(place, sub).wait_send()

        @pl.when((place >= z) & jnp.logical_not(lowest))
        def _():
            down_copy(place, sub).wait_send()

        return carry

    def drain_all():
        lax.fori_loop(0, units, drain, 0)

        def sent(view, semaphore):
            remote(view, view, semaphore, semaphore, partner, tp).wait_send()

        def column(buffer, count, extent):
            return buffer.at[pl.ds(0, count), pl.ds(0, extent)]

        sent(tokens.at[pl.ds(0, rows * chips)], core_send.at[0])
        sent(half_out, half_send.at[0])
        sent(result.at[pl.ds(0, units - SPLIT)], result_send.at[0])
        sent(shares.at[pl.ds(0, n - 1)], share_send.at[0])
        for k in direct:
            sent(column(hidden, n * rows, part), hidden_send.at[k])
            sent(column(heads, length, spread), head_send.at[k])
        if square:
            for way in range(2):
                sent(column(hidden, chips * rows, part), pass_send.at[way])
                head_forward(way).wait_send()

        @pl.when(jnp.logical_not(last))
        def _():
            edge_copy(0).wait_send()

        @pl.when(jnp.logical_not(first))
        def _():
            edge_copy(1).wait_send()

    units = chips * SPLIT

    def step(index, carry):
        hop, sub = 1 + index // SPLIT, index % SPLIT
        arrive(hop, sub)
        sides(hop, lambda place, k: first_half(unit(place, sub)))

        @pl.when(index == 0)
        def _():
            for own_sub in range(1, SPLIT):
                hidden_pass(unit(z, own_sub))

        @pl.when(index > 0)
        def _():
            one(index - 1, hidden_pass)

        @pl.when(index > 1)
        def _():
            two(index - 2, hidden_pass)

        @pl.when((index >= look) & (index < look + 2))
        def _():
            attention(index - look)

        @pl.when((index == 3) & ending)
        def _():
            head_pass()

        @pl.when(index > 2)
        def _():
            one(index - 3, deliver)

        @pl.when(index > 1)
        def _():
            one(index - 2, second_half)

        @pl.when(index > 3)
        def _():
            two(index - 4, deliver)

        @pl.when(index > 2)
        def _():
            two(index - 3, second_half)

        return carry

    loads[7].wait()
    lax.fori_loop(0, n, spread_shares, 0)
    hidden_pass(unit(z, 0))
    lax.fori_loop(0, steps, step, 0)
    loads[8].wait()
    second_half(unit(z, 0))
    one(steps - 1, hidden_pass)
    two(steps - 2, hidden_pass)
    two(steps - 1, hidden_pass)
    one(steps - 3, deliver)
    two(steps - 4, deliver)
    for sub in range(1, SPLIT):
        second_half(unit(z, sub))
    one(steps - 2, second_half)
    two(steps - 3, second_half)

    @pl.when(ending)
    def _():
        project()

    two(steps - 3, deliver)
    one(steps - 2, deliver)
    one(steps - 1, second_half)
    two(steps - 2, second_half)
    two(steps - 1, second_half)
    one(steps - 1, deliver)
    two(steps - 2, deliver)
    two(steps - 1, deliver)

    @pl.when(jnp.logical_not(ending))
    def _():
        head_pass()
        project()

    own_units(combine)
    drain_all()

    for sub in range(SPLIT):
        total = result[unit(z, sub)].astype(jnp.float32)
        for k in range(1, chips):
            source = lax.rem(z + k, chips)
            result_copy(unit(source, sub), source).wait_recv()
            total += returned[source, sub].astype(jnp.float32)
        expert_out[sub * size : (sub + 1) * size, :] = total.astype(jnp.bfloat16)


def settle(first_ref, second_ref, first_out, second_out):
    first_out[...] = first_ref[...]
    second_out[...] = second_ref[...]


def shards(
    mixer_input,
    mixer_gain,
    query_weight,
    key_weight,
    value_weight,
    output_weight,
    sink_logit,
    expert_input,
    expert_gain,
    routes,
    route_logits,
    gate_weight,
    up_weight,
    down_weight,
):
    tokens = mixer_input.shape[0]
    lanes = 2 * HEAD_DIM
    quarter = HEAD_DIM // 4
    spot = np.arange(lanes) % quarter
    frequency = (BASE ** (-spot.astype(np.float32) / np.float32(quarter))).astype(np.float32)[None]
    experts = lax.axis_size("ep")
    parts = lax.axis_size("tp")
    rows, width = expert_input.shape
    part = gate_weight.shape[2]
    vmem = pl.BlockSpec(memory_space=pltpu.VMEM)
    outside = pl.BlockSpec(memory_space=pltpu.HBM)
    chips = experts // 2
    dma = pltpu.SemaphoreType.DMA
    columns = down_weight.shape[2]
    spread = query_weight.shape[1]
    half = jnp.bfloat16
    size, units = rows // SPLIT, chips * SPLIT
    results = pl.pallas_call(
        functools.partial(exchange, experts, parts),
        out_shape=(
            jax.ShapeDtypeStruct((tokens, output_weight.shape[1]), half),
            jax.ShapeDtypeStruct((rows, columns), half),
        ),
        in_specs=[outside] * 15,
        out_specs=(vmem, vmem),
        scratch_shapes=[
            pltpu.VMEM((1, width), jnp.float32),
            pltpu.VMEM((TOP_K, rows), jnp.float32),
            pltpu.VMEM((TOP_K, rows), jnp.int32),
            pltpu.VMEM((1, width), jnp.float32),
            pltpu.VMEM((1, lanes), jnp.float32),
            pltpu.VMEM((1, sink_logit.shape[0]), jnp.float32),
            pltpu.VMEM((rows, width), half),
            pltpu.VMEM(mixer_input.shape, half),
            pltpu.VMEM((experts * rows, width), half),
            pltpu.VMEM((experts * rows, parts * part), half),
            pltpu.VMEM((tokens, parts * spread), half),
            pltpu.VMEM((experts, experts, rows), jnp.float32),
            pltpu.VMEM((units, size, columns), half),
            pltpu.VMEM((units, size, columns), half),
            pltpu.VMEM((units, size, columns), half),
            pltpu.VMEM((chips, SPLIT, size, columns), half),
            pltpu.VMEM((units, 2 * size, columns), jnp.float32),
            pltpu.VMEM((experts * rows, rows), jnp.float32),
            pltpu.VMEM((tokens, lanes), jnp.float32),
            pltpu.VMEM((tokens, lanes), jnp.float32),
            pltpu.VMEM((tokens, spread), half),
            pltpu.VMEM((tokens + 2 * WINDOW, 2 * key_weight.shape[1]), half),
            pltpu.VMEM(query_weight.shape, half),
            pltpu.VMEM(key_weight.shape, half),
            pltpu.VMEM(value_weight.shape, half),
            pltpu.VMEM(output_weight.shape, half),
            pltpu.VMEM(gate_weight.shape[1:], half),
            pltpu.VMEM(up_weight.shape[1:], half),
            pltpu.VMEM(down_weight.shape[1:], half),
            dma((15,)),
            dma((2 * units,)),
            dma((units,)),
            dma((units,)),
            dma((1,)),
            dma((parts,)),
            dma((parts, units, 2)),
            dma((2,)),
            dma((parts,)),
            dma((parts, 2)),
            dma((2,)),
            dma((2,)),
            dma((2,)),
            dma((1,)),
            dma((experts,)),
            dma((1,)),
            dma((units,)),
            dma((1,)),
            dma((chips, SPLIT)),
        ],
        compiler_params=pltpu.CompilerParams(
            collective_id=0, has_side_effects=True, vmem_limit_bytes=60 * 1024 * 1024
        ),
    )(
        expert_input,
        expert_gain.reshape(1, -1),
        route_logits.T,
        routes.T,
        mixer_input,
        mixer_gain.reshape(1, -1),
        jnp.asarray(frequency),
        sink_logit.reshape(1, -1),
        query_weight,
        key_weight,
        value_weight,
        output_weight,
        gate_weight[0],
        up_weight[0],
        down_weight[0],
    )
    return pl.pallas_call(
        settle,
        out_shape=tuple(jax.ShapeDtypeStruct(r.shape, r.dtype) for r in results),
        in_specs=[vmem, vmem],
        out_specs=(vmem, vmem),
    )(*results)


def solution(mesh):
    return jax.shard_map(
        shards,
        mesh=mesh,
        in_specs=(
            P("ep", None),
            P(),
            P(None, "tp"),
            P(None, "tp"),
            P(None, "tp"),
            P(None, "tp"),
            P("tp"),
            P("ep", None),
            P(),
            P("ep", None),
            P("ep", None),
            P("ep", None, "tp"),
            P("ep", None, "tp"),
            P("ep", None, "tp"),
        ),
        out_specs=(P("ep", "tp"), P("ep", "tp")),
        check_vma=False,
    )
```

```python
import functools

import jax
import jax.numpy as jnp
import numpy as np
from jax import lax
from jax.experimental import pallas as pl
from jax.experimental.pallas import tpu as pltpu
from jax.sharding import PartitionSpec as P

HEAD_DIM = 64
TOP_K = 4
WINDOW = 128
GRID_W = 64
SPLIT = 2
EARLY = 0
LATE = 3


EPSILON = 1e-06
LIMIT = 7.0
SLOPE = 1.702
BASE = 10000.0


def normalize(rows, gain):
    values = rows.astype(jnp.float32)
    scaled = values * lax.rsqrt(jnp.mean(values * values, axis=-1, keepdims=True) + EPSILON)
    return (scaled * gain).astype(jnp.bfloat16)


def rotate(values, cosine, sine):
    width = values.shape[1]
    lanes = cosine.shape[1]
    if width < lanes:
        return rotate(jnp.concatenate([values] * (lanes // width), axis=1), cosine, sine)[:, :width]
    spot = lax.broadcasted_iota(jnp.int32, cosine.shape, 1)
    leading = spot % (HEAD_DIM // 2) < HEAD_DIM // 4
    pieces = []
    for start in range(0, width, lanes):
        piece = values[:, start : start + lanes]
        other = jnp.where(
            leading,
            pltpu.roll(piece, lanes - HEAD_DIM // 4, 1),
            pltpu.roll(piece, HEAD_DIM // 4, 1),
        )
        pieces.append(piece * cosine + other * sine)
    return jnp.concatenate(pieces, axis=1)


def activate(gate, up):
    capped = jnp.minimum(gate, LIMIT)
    bounded = jnp.clip(up, -LIMIT, LIMIT)
    return (capped * jax.nn.sigmoid(SLOPE * capped) * (bounded + 1.0)).astype(jnp.bfloat16)


def remote(src, dst, sent, landed, ep, tp):
    return pltpu.make_async_remote_copy(
        src_ref=src,
        dst_ref=dst,
        send_sem=sent,
        recv_sem=landed,
        device_id=(ep, tp),
        device_id_type=pl.DeviceIdType.MESH,
    )


def exchange(
    n,
    t,
    x_hbm,
    gain_hbm,
    logit_hbm,
    route_hbm,
    mixer_hbm,
    mixer_gain_hbm,
    frequency_hbm,
    sink_hbm,
    wq_hbm,
    wk_hbm,
    wv_hbm,
    wo_hbm,
    wg_hbm,
    wu_hbm,
    wd_hbm,
    mixer_hbm_out,
    expert_hbm_out,
    mixer_out,
    expert_out,
    gain_ref,
    logit_ref,
    route_ref,
    mixer_gain_ref,
    frequency_ref,
    sink_ref,
    x_ref,
    mixer_ref,
    tokens,
    hidden,
    heads,
    shares,
    half_out,
    half_in,
    result,
    returned,
    kept_half,
    scales,
    cosine_ref,
    sine_ref,
    lent,
    queries,
    around,
    wq,
    wk,
    wv,
    wo,
    wg,
    wu,
    wd,
    local_sem,
    out_sem,
    token_recv,
    up_send,
    down_send,
    core_send,
    hidden_send,
    hidden_recv,
    pass_send,
    head_send,
    head_recv,
    head_pass_send,
    edge_send,
    edge_recv,
    lent_send,
    lent_recv,
    share_send,
    share_recv,
    half_send,
    half_recv,
    result_send,
    result_recv,
):
    ep, tp = lax.axis_index("ep"), lax.axis_index("tp")
    chips = n // 2
    z, core = ep // 2, ep % 2
    partner = 2 * z + 1 - core
    rows = x_ref.shape[0]
    size = rows // SPLIT
    pair = 2 * size
    part = wg.shape[1]
    length = mixer_ref.shape[0]
    kept = wk.shape[1]
    spread = wq.shape[1]
    square = t == 4
    direct = (1, 2) if square else tuple(range(1, t))

    def peer(k):
        if not square:
            return lax.rem(tp + k, t)
        return lax.rem(tp + (k // 2) * 2 + (k % 2) * (1 - 2 * (tp % 2)) + t, t)

    def block(index, size):
        return pl.ds(pl.multiple_of(index * size, size), size)

    loads = [
        pltpu.make_async_copy(a, b, local_sem.at[i])
        for i, (a, b) in enumerate((
            (x_hbm, x_ref),
            (wg_hbm, wg),
            (wu_hbm, wu),
            (mixer_hbm, mixer_ref),
            (wk_hbm, wk),
            (wv_hbm, wv),
            (wq_hbm, wq),
            (wd_hbm, wd),
            (wo_hbm, wo),
            (frequency_hbm, frequency_ref),
            (logit_hbm, logit_ref),
            (route_hbm, route_ref),
            (gain_hbm, gain_ref),
            (mixer_gain_hbm, mixer_gain_ref),
            (sink_hbm, sink_ref),
        ))
    ]
    for load in loads[9:] + loads[:9]:
        load.start()

    barrier = pltpu.get_barrier_semaphore()
    for k in range(1, n):
        pl.semaphore_signal(
            barrier,
            inc=1,
            device_id=(lax.rem(ep + k, n), tp),
            device_id_type=pl.DeviceIdType.MESH,
        )
    for k in range(1, t):
        pl.semaphore_signal(
            barrier,
            inc=1,
            device_id=(ep, peer(k)),
            device_id_type=pl.DeviceIdType.MESH,
        )

    for load in loads[9:]:
        load.wait()
    logits = logit_ref[...]
    raised = jnp.exp(logits - jnp.max(logits, axis=0, keepdims=True))
    chances = raised / jnp.sum(raised, axis=0, keepdims=True)
    number = lax.broadcasted_iota(jnp.int32, (n, rows), 0)
    share = jnp.zeros((n, rows), jnp.float32)
    for k in range(TOP_K):
        share += jnp.where(route_ref[k : k + 1, :] == number, chances[k : k + 1, :], 0.0)
    shares[ep] = share

    lanes = 2 * HEAD_DIM
    spot = lax.broadcasted_iota(jnp.int32, (length, lanes), 1)
    token = ep * length + lax.broadcasted_iota(jnp.int32, (length, lanes), 0)
    turn = jnp.where(spot % HEAD_DIM < HEAD_DIM // 2, token // GRID_W, token % GRID_W)
    turn = turn.astype(jnp.float32) * frequency_ref[...]
    cosine_ref[...] = jnp.cos(turn)
    sine_ref[...] = jnp.sin(turn) * jnp.where(spot % (HEAD_DIM // 2) < HEAD_DIM // 4, -1.0, 1.0)

    loads[0].wait()
    fresh = normalize(x_ref[...], gain_ref[...])
    for sub in range(SPLIT):
        inside = block(2 * (z * SPLIT + sub) + core, size)
        tokens[inside, :] = fresh[sub * size : (sub + 1) * size]

    def unit(place, sub):
        return place * SPLIT + sub

    def token_copy(slot, sent, target):
        piece = tokens.at[block(slot, size)]
        return remote(piece, piece, sent, token_recv.at[slot], target, tp)

    def up_copy(place, sub):
        u = unit(place, sub)
        return token_copy(2 * u + core, up_send.at[u], ep + 2)

    def down_copy(place, sub):
        u = unit(place, sub)
        return token_copy(2 * u + core, down_send.at[u], ep - 2)

    def core_copy(place, sub):
        u = unit(place, sub)
        return token_copy(2 * u + core, core_send.at[0], partner)

    def token_wait(slot):
        token_copy(slot, core_send.at[0], partner).wait_recv()

    def share_copy(k):
        piece = shares.at[ep]
        target = lax.rem(ep + k, n)
        return remote(piece, piece, share_send.at[0], share_recv.at[0], target, tp)

    def share_wait():
        piece = shares.at[pl.ds(0, n - 1)]
        remote(piece, piece, share_send.at[0], share_recv.at[0], partner, tp).wait_recv()

    lowest, highest = z == 0, z == chips - 1

    def spread_own(sub):
        @pl.when(jnp.logical_not(highest))
        def _():
            up_copy(z, sub).start()

        @pl.when(jnp.logical_not(lowest))
        def _():
            down_copy(z, sub).start()

    def hidden_piece(source, u, half):
        return hidden.at[
            block(2 * u + half, size), pl.ds(pl.multiple_of(source * part, part), part)
        ]

    def kind_of(k, half):
        if square and k < 3:
            return jnp.where(half == k - 1, k - 1, 2)
        return 2

    def hidden_copy(source, u, half, k):
        piece = hidden_piece(source, u, half)
        return remote(
            piece,
            piece,
            hidden_send.at[k],
            hidden_recv.at[u, kind_of(k, half)],
            ep,
            peer(k),
        )

    def hidden_forward(u, way):
        source = peer(2 - way)
        piece = hidden_piece(source, u, 1 - way)
        return remote(
            piece,
            piece,
            pass_send.at[way],
            hidden_recv.at[u, 2],
            ep,
            peer(1 + way),
        )

    def hidden_pass(u):
        if square:
            for way in range(2):
                hidden_copy(peer(2 - way), u, 1 - way, 2 - way).wait_recv()
                hidden_forward(u, way).start()

    others = 2 if square else t - 1

    def hidden_wait(u):
        view = hidden.at[pl.ds(0, pair), pl.ds(0, others * part)]
        remote(view, view, hidden_send.at[0], hidden_recv.at[u, 2], ep, peer(1)).wait_recv()

    def head_piece(source, half):
        return heads.at[
            block(half, length // 2),
            pl.ds(pl.multiple_of(source * spread, spread), spread),
        ]

    def head_copy(source, half, k):
        piece = head_piece(source, half)
        return remote(
            piece, piece, head_send.at[k], head_recv.at[kind_of(k, half)], ep, peer(k)
        )

    def head_forward(way):
        source = peer(2 - way)
        piece = head_piece(source, 1 - way)
        return remote(
            piece,
            piece,
            head_pass_send.at[way],
            head_recv.at[2],
            ep,
            peer(1 + way),
        )

    def head_pass():
        if square:
            for way in range(2):
                head_copy(peer(2 - way), 1 - way, 2 - way).wait_recv()
                head_forward(way).start()

    def head_wait():
        view = heads.at[:, pl.ds(0, others * spread)]
        remote(view, view, head_send.at[0], head_recv.at[2], ep, peer(1)).wait_recv()

    def expand(slots):
        span = min(256, part)
        for start in range(0, part, span):
            cut = slice(start, start + span)
            lines = jnp.concatenate([tokens[block(slot, size), :] for slot in slots], axis=0)
            gate = jnp.dot(lines, wg[:, cut], preferred_element_type=jnp.float32)
            up = jnp.dot(lines, wu[:, cut], preferred_element_type=jnp.float32)
            column = pl.ds(pl.multiple_of(tp * part + start, span), span)
            active = activate(gate, up)
            for i, slot in enumerate(slots):
                hidden[block(slot, size), column] = active[i * size : (i + 1) * size]

    def first_half(u):
        token_wait(2 * u + 1 - core)
        expand([2 * u, 2 * u + 1])
        for order in range(2):
            for k in direct:
                hidden_copy(tp, u, order if k != 2 else 1 - order, k).start()

    def first_own(side):
        expand([2 * unit(z, sub) + side for sub in range(SPLIT)])

    def send_own(side):
        for sub in range(SPLIT):
            for k in direct:
                hidden_copy(tp, unit(z, sub), side, k).start()

    pl.semaphore_wait(barrier, n + t - 2)
    for k in range(1, n):
        share_copy(k).start()
    spread_own(0)
    for sub in range(SPLIT):
        core_copy(z, sub).start()
    loads[1].wait()
    loads[2].wait()
    first_own(core)
    send_own(core)

    loads[3].wait()
    normed = normalize(mixer_ref[...], mixer_gain_ref[...])
    own = slice(WINDOW, WINDOW + length)
    for load in loads[4:6]:
        load.wait()
    cosine, sine = cosine_ref[...], sine_ref[...]
    keys = jnp.dot(normed, wk[...], preferred_element_type=jnp.float32)
    around[own, 0:kept] = rotate(keys, cosine, sine).astype(jnp.bfloat16)
    around[own, kept:] = jnp.dot(normed, wv[...], preferred_element_type=jnp.float32).astype(
        jnp.bfloat16
    )

    reach = WINDOW // 2

    def edge_copy(way, part_of):
        source, target = (length, 0) if way == 0 else (WINDOW, WINDOW + length)
        return remote(
            around.at[pl.ds(source + part_of * reach, reach)],
            around.at[pl.ds(target + part_of * reach, reach)],
            edge_send.at[way, part_of],
            edge_recv.at[way, part_of],
            ep + (1 if way == 0 else -1),
            tp,
        )

    def lend_copy(way):
        source = length if way == 0 else WINDOW
        return remote(
            around.at[pl.ds(source + reach, reach)],
            lent,
            edge_send.at[way, 1],
            lent_recv.at[0],
            partner,
            tp,
        )

    def lent_copy(way):
        target = 0 if way == 0 else WINDOW + length
        return remote(
            lent,
            around.at[pl.ds(target + reach, reach)],
            lent_send.at[0],
            edge_recv.at[way, 1],
            partner + (1 if way == 0 else -1),
            tp,
        )

    first, last = ep == 0, ep == n - 1

    crossing = ((core == 1) & jnp.logical_not(highest), (core == 0) & jnp.logical_not(lowest))
    lending = ((core == 0) & jnp.logical_not(highest), (core == 1) & jnp.logical_not(lowest))
    for way in range(2):
        @pl.when(core == way)
        def _():
            for part_of in range(2):
                edge_copy(way, part_of).start()

        @pl.when(crossing[way])
        def _():
            lend_copy(way).start()
            edge_copy(way, 0).start()

    for sub in range(1, SPLIT):
        spread_own(sub)

    @pl.when(first)
    def _():
        around[0:WINDOW, :] = jnp.zeros((WINDOW, around.shape[1]), jnp.bfloat16)

    @pl.when(last)
    def _():
        around[WINDOW + length :, :] = jnp.zeros((WINDOW, around.shape[1]), jnp.bfloat16)

    for sub in range(SPLIT):
        token_wait(2 * unit(z, sub) + 1 - core)
    first_own(1 - core)
    send_own(1 - core)

    for way in range(2):
        @pl.when(lending[way])
        def _():
            lend_copy(way).wait_recv()
            lent_copy(way).start()

    loads[6].wait()
    turned = jnp.dot(normed, wq[...], preferred_element_type=jnp.float32)
    queries[...] = rotate(turned, cosine, sine).astype(jnp.bfloat16)

    def attend(number, carry):
        inside = pl.ds(pl.multiple_of(number * WINDOW, WINDOW), WINDOW)
        seen = pl.ds(pl.multiple_of(number * WINDOW, WINDOW), 3 * WINDOW)
        shape = (WINDOW, 3 * WINDOW)
        line = lax.broadcasted_iota(jnp.int32, shape, 0)
        key = lax.broadcasted_iota(jnp.int32, shape, 1)
        place = ep * length + (number - 1) * WINDOW + key
        allowed = (key >= line) & (key <= line + 2 * WINDOW) & (place >= 0) & (place < n * length)
        group = queries.shape[1] // kept
        allowed = jnp.concatenate([allowed] * group, axis=0)
        for head in range(kept // HEAD_DIM):
            first = head * group
            query = jnp.concatenate(
                [
                    queries[inside, (first + r) * HEAD_DIM : (first + r + 1) * HEAD_DIM]
                    for r in range(group)
                ],
                axis=0,
            )
            sinks = jnp.concatenate(
                [
                    jnp.broadcast_to(sink_ref[:, first + r : first + r + 1], (WINDOW, 1))
                    for r in range(group)
                ],
                axis=0,
            )
            near_keys = around[seen, head * HEAD_DIM : (head + 1) * HEAD_DIM]
            near_values = around[seen, kept + head * HEAD_DIM : kept + (head + 1) * HEAD_DIM]
            scores = lax.dot_general(
                query,
                near_keys,
                (((1,), (1,)), ((), ())),
                preferred_element_type=jnp.float32,
            ) * HEAD_DIM ** (-0.5)
            scores = jnp.where(allowed, scores, -1e30)
            top = jnp.maximum(jnp.max(scores, axis=-1, keepdims=True), sinks)
            weights = jnp.exp(scores - top)
            denominator = jnp.sum(weights, axis=-1, keepdims=True) + jnp.exp(sinks - top)
            share = (weights * (1.0 / denominator)).astype(jnp.bfloat16)
            mixed = jnp.dot(share, near_values, preferred_element_type=jnp.float32)
            mixed = mixed.astype(jnp.bfloat16)
            width = group * HEAD_DIM
            column = pl.ds(pl.multiple_of(tp * spread + first * HEAD_DIM, width), width)
            heads[inside, column] = jnp.concatenate(
                [mixed[r * WINDOW : (r + 1) * WINDOW] for r in range(group)], axis=1
            )
        return carry

    def attention(half):
        for way in range(2):
            @pl.when((half == way) & jnp.logical_not(first if way == 0 else last))
            def _():
                for part_of in range(2):
                    edge_copy(way, part_of).wait_recv()

        count = length // 2 // WINDOW
        lax.fori_loop(half * count, (half + 1) * count, attend, 0)
        for k in direct:
            head_copy(tp, half, k).start()

    def half_copy(u):
        return remote(
            half_out.at[u], half_in.at[u], half_send.at[0], half_recv.at[u], partner, tp
        )

    def result_copy(u, source):
        return remote(
            result.at[u],
            returned.at[source, u % SPLIT],
            result_send.at[0],
            result_recv.at[u % SPLIT],
            2 * (u // SPLIT) + core,
            tp,
        )

    def spread_shares(slot, carry):
        line = shares[slot, pl.ds(ep, 1), :]
        column = jnp.transpose(jnp.broadcast_to(line, (rows, rows)))
        for sub in range(SPLIT):
            inside = block(2 * unit(slot // 2, sub) + slot % 2, size)
            scales[inside, :] = column[sub * size : (sub + 1) * size]
        return carry

    def second_half(u):
        hidden_wait(u)
        inside = block(u, pair)
        total = jnp.dot(hidden[inside, :], wd[...], preferred_element_type=jnp.float32)
        column = scales[inside, :]
        kept_half[u] = jnp.concatenate(
            [total[:, i : i + rows] * column for i in range(0, total.shape[1], rows)], axis=1
        )
        half_out[u] = kept_half[u, block(1 - core, size), :].astype(jnp.bfloat16)
        half_copy(u).start()

    def combine(u):
        half_copy(u).wait_recv()
        total = kept_half[u, block(core, size), :] + half_in[u].astype(jnp.float32)
        result[u] = total.astype(jnp.bfloat16)

    def sides(hop, action):
        def side(k, carry):
            place = z + (2 * k - 1) * hop

            @pl.when((place >= 0) & (place < chips))
            def _():
                action(place, k)

            return carry

        lax.fori_loop(0, 2, side, 0)

    def arrive(hop, sub):
        below, above = z - hop, z + hop

        @pl.when(below >= 0)
        def _():
            token_wait(2 * unit(below, sub) + core)

            @pl.when(jnp.logical_not(highest))
            def _():
                up_copy(below, sub).start()

            core_copy(below, sub).start()

        @pl.when(above < chips)
        def _():
            token_wait(2 * unit(above, sub) + core)

            @pl.when(jnp.logical_not(lowest))
            def _():
                down_copy(above, sub).start()

            core_copy(above, sub).start()

    steps = (chips - 1) * SPLIT

    def one(index, action):
        hop, sub = 1 + index // SPLIT, index % SPLIT
        below, above = z - hop, z + hop

        @pl.when((below >= 0) | (above < chips))
        def _():
            action(unit(jnp.where(below >= 0, below, above), sub))

    def two(index, action):
        hop, sub = 1 + index // SPLIT, index % SPLIT
        below, above = z - hop, z + hop

        @pl.when((below >= 0) & (above < chips))
        def _():
            action(unit(above, sub))

    def deliver(u):
        combine(u)
        result_copy(u, z).start()

    ending = lowest | highest
    look = jnp.where(ending, EARLY, LATE)

    def own_units(action):
        for sub in range(SPLIT):
            action(unit(z, sub))

    mixer_store = pltpu.make_async_copy(mixer_out, mixer_hbm_out, out_sem.at[SPLIT])

    def expert_store(sub):
        inside = pl.ds(sub * size, size)
        return pltpu.make_async_copy(expert_out.at[inside], expert_hbm_out.at[inside], out_sem.at[sub])

    def project():
        head_wait()
        mixer_out[...] = jnp.dot(heads[...], wo[...], preferred_element_type=jnp.float32).astype(
            jnp.bfloat16
        )
        mixer_store.start()

    def drain(u, carry):
        place, sub = u // SPLIT, u % SPLIT

        @pl.when((place <= z) & jnp.logical_not(highest))
        def _():
            up_copy(place, sub).wait_send()

        @pl.when((place >= z) & jnp.logical_not(lowest))
        def _():
            down_copy(place, sub).wait_send()

        return carry

    def drain_all():
        lax.fori_loop(0, units, drain, 0)

        def sent(view, semaphore):
            remote(view, view, semaphore, semaphore, partner, tp).wait_send()

        def column(buffer, count, extent):
            return buffer.at[pl.ds(0, count), pl.ds(0, extent)]

        sent(tokens.at[pl.ds(0, rows * chips)], core_send.at[0])
        sent(half_out, half_send.at[0])
        sent(result.at[pl.ds(0, units - SPLIT)], result_send.at[0])
        sent(shares.at[pl.ds(0, n - 1)], share_send.at[0])
        for k in direct:
            sent(column(hidden, n * rows, part), hidden_send.at[k])
            sent(column(heads, length, spread), head_send.at[k])
        if square:
            for way in range(2):
                sent(column(hidden, chips * rows, part), pass_send.at[way])
                head_forward(way).wait_send()

        for way in range(2):
            @pl.when((core == way) | crossing[way])
            def _():
                for part_of in range(2):
                    edge_copy(way, part_of).wait_send()

            @pl.when(lending[way])
            def _():
                lent_copy(way).wait_send()

    units = chips * SPLIT

    def step(index, carry):
        hop, sub = 1 + index // SPLIT, index % SPLIT
        arrive(hop, sub)
        sides(hop, lambda place, k: first_half(unit(place, sub)))

        @pl.when(index == 0)
        def _():
            for own_sub in range(1, SPLIT):
                hidden_pass(unit(z, own_sub))

        @pl.when(index > 0)
        def _():
            one(index - 1, hidden_pass)

        @pl.when(index > 1)
        def _():
            two(index - 2, hidden_pass)

        @pl.when((index >= look) & (index < look + 2))
        def _():
            attention(jnp.where(highest, 1 - (index - look), index - look))

        @pl.when((index == 3) & ending)
        def _():
            head_pass()

        @pl.when(index > 2)
        def _():
            one(index - 3, deliver)

        @pl.when(index > 1)
        def _():
            one(index - 2, second_half)

        @pl.when(index > 3)
        def _():
            two(index - 4, deliver)

        @pl.when(index > 2)
        def _():
            two(index - 3, second_half)

        return carry

    loads[7].wait()
    share_wait()
    lax.fori_loop(0, n, spread_shares, 0)
    hidden_pass(unit(z, 0))
    lax.fori_loop(0, steps, step, 0)
    loads[8].wait()
    second_half(unit(z, 0))
    one(steps - 1, hidden_pass)
    two(steps - 2, hidden_pass)
    two(steps - 1, hidden_pass)
    for sub in range(1, SPLIT):
        second_half(unit(z, sub))
    one(steps - 3, deliver)
    two(steps - 4, deliver)
    @pl.when(ending)
    def _():
        project()

    one(steps - 2, second_half)
    two(steps - 3, second_half)
    one(steps - 2, deliver)
    two(steps - 3, deliver)

    one(steps - 1, second_half)
    two(steps - 2, second_half)
    two(steps - 1, second_half)
    one(steps - 1, deliver)
    two(steps - 2, deliver)
    two(steps - 1, deliver)

    @pl.when(jnp.logical_not(ending))
    def _():
        head_pass()
        project()

    own_units(combine)
    drain_all()

    for sub in range(SPLIT):
        total = result[unit(z, sub)].astype(jnp.float32)
        view = result.at[pl.ds(0, chips - 1)]
        remote(view, view, result_send.at[0], result_recv.at[sub], partner, tp).wait_recv()
        for k in range(1, chips):
            source = lax.rem(z + k, chips)
            total += returned[source, sub].astype(jnp.float32)
        expert_out[sub * size : (sub + 1) * size, :] = total.astype(jnp.bfloat16)
        expert_store(sub).start()

    for sub in range(SPLIT):
        expert_store(sub).wait()
    mixer_store.wait()


def settle(first_ref, second_ref, first_out, second_out):
    first_out[...] = first_ref[...]
    second_out[...] = second_ref[...]


def shards(
    mixer_input,
    mixer_gain,
    query_weight,
    key_weight,
    value_weight,
    output_weight,
    sink_logit,
    expert_input,
    expert_gain,
    routes,
    route_logits,
    gate_weight,
    up_weight,
    down_weight,
):
    tokens = mixer_input.shape[0]
    lanes = 2 * HEAD_DIM
    quarter = HEAD_DIM // 4
    spot = np.arange(lanes) % quarter
    frequency = (BASE ** (-spot.astype(np.float32) / np.float32(quarter))).astype(np.float32)[None]
    experts = lax.axis_size("ep")
    parts = lax.axis_size("tp")
    rows, width = expert_input.shape
    part = gate_weight.shape[2]
    vmem = pl.BlockSpec(memory_space=pltpu.VMEM)
    outside = pl.BlockSpec(memory_space=pltpu.HBM)
    chips = experts // 2
    dma = pltpu.SemaphoreType.DMA
    columns = down_weight.shape[2]
    spread = query_weight.shape[1]
    half = jnp.bfloat16
    size, units = rows // SPLIT, chips * SPLIT
    results = pl.pallas_call(
        functools.partial(exchange, experts, parts),
        out_shape=(
            jax.ShapeDtypeStruct((tokens, output_weight.shape[1]), half),
            jax.ShapeDtypeStruct((rows, columns), half),
        ),
        in_specs=[outside] * 15,
        out_specs=(outside, outside),
        scratch_shapes=[
            pltpu.VMEM((tokens, output_weight.shape[1]), half),
            pltpu.VMEM((rows, columns), half),
            pltpu.VMEM((1, width), jnp.float32),
            pltpu.VMEM((TOP_K, rows), jnp.float32),
            pltpu.VMEM((TOP_K, rows), jnp.int32),
            pltpu.VMEM((1, width), jnp.float32),
            pltpu.VMEM((1, lanes), jnp.float32),
            pltpu.VMEM((1, sink_logit.shape[0]), jnp.float32),
            pltpu.VMEM((rows, width), half),
            pltpu.VMEM(mixer_input.shape, half),
            pltpu.VMEM((experts * rows, width), half),
            pltpu.VMEM((experts * rows, parts * part), half),
            pltpu.VMEM((tokens, parts * spread), half),
            pltpu.VMEM((experts, experts, rows), jnp.float32),
            pltpu.VMEM((units, size, columns), half),
            pltpu.VMEM((units, size, columns), half),
            pltpu.VMEM((units, size, columns), half),
            pltpu.VMEM((chips, SPLIT, size, columns), half),
            pltpu.VMEM((units, 2 * size, columns), jnp.float32),
            pltpu.VMEM((experts * rows, rows), jnp.float32),
            pltpu.VMEM((tokens, lanes), jnp.float32),
            pltpu.VMEM((tokens, lanes), jnp.float32),
            pltpu.VMEM((WINDOW // 2, 2 * key_weight.shape[1]), half),
            pltpu.VMEM((tokens, spread), half),
            pltpu.VMEM((tokens + 2 * WINDOW, 2 * key_weight.shape[1]), half),
            pltpu.VMEM(query_weight.shape, half),
            pltpu.VMEM(key_weight.shape, half),
            pltpu.VMEM(value_weight.shape, half),
            pltpu.VMEM(output_weight.shape, half),
            pltpu.VMEM(gate_weight.shape[1:], half),
            pltpu.VMEM(up_weight.shape[1:], half),
            pltpu.VMEM(down_weight.shape[1:], half),
            dma((15,)),
            dma((SPLIT + 1,)),
            dma((2 * units,)),
            dma((units,)),
            dma((units,)),
            dma((1,)),
            dma((parts,)),
            dma((units, 3)),
            dma((2,)),
            dma((parts,)),
            dma((3,)),
            dma((2,)),
            dma((2, 2)),
            dma((2, 2)),
            dma((1,)),
            dma((1,)),
            dma((1,)),
            dma((1,)),
            dma((1,)),
            dma((units,)),
            dma((1,)),
            dma((SPLIT,)),
        ],
        compiler_params=pltpu.CompilerParams(
            collective_id=0, has_side_effects=True, vmem_limit_bytes=60 * 1024 * 1024
        ),
    )(
        expert_input,
        expert_gain.reshape(1, -1),
        route_logits.T,
        routes.T,
        mixer_input,
        mixer_gain.reshape(1, -1),
        jnp.asarray(frequency),
        sink_logit.reshape(1, -1),
        query_weight,
        key_weight,
        value_weight,
        output_weight,
        gate_weight[0],
        up_weight[0],
        down_weight[0],
    )
    return pl.pallas_call(
        settle,
        out_shape=tuple(jax.ShapeDtypeStruct(r.shape, r.dtype) for r in results),
        in_specs=[vmem, vmem],
        out_specs=(vmem, vmem),
    )(*results)


def solution(mesh):
    return jax.shard_map(
        shards,
        mesh=mesh,
        in_specs=(
            P("ep", None),
            P(),
            P(None, "tp"),
            P(None, "tp"),
            P(None, "tp"),
            P(None, "tp"),
            P("tp"),
            P("ep", None),
            P(),
            P("ep", None),
            P("ep", None),
            P("ep", None, "tp"),
            P("ep", None, "tp"),
            P("ep", None, "tp"),
        ),
        out_specs=(P("ep", "tp"), P("ep", "tp")),
        check_vma=False,
    )
```

```python
import functools

import jax
import jax.numpy as jnp
import numpy as np
from jax import lax
from jax.experimental import pallas as pl
from jax.experimental.pallas import tpu as pltpu
from jax.sharding import PartitionSpec as P

HEAD_DIM = 64
TOP_K = 4
WINDOW = 128
GRID_W = 64
SPLIT = 2
EARLY = 0
LATE = 3


EPSILON = 1e-06
LIMIT = 7.0
SLOPE = 1.702
BASE = 10000.0


def normalize(rows, gain):
    values = rows.astype(jnp.float32)
    scaled = values * lax.rsqrt(jnp.mean(values * values, axis=-1, keepdims=True) + EPSILON)
    return (scaled * gain).astype(jnp.bfloat16)


def rotate(values, cosine, sine):
    width = values.shape[1]
    lanes = cosine.shape[1]
    if width < lanes:
        return rotate(jnp.concatenate([values] * (lanes // width), axis=1), cosine, sine)[:, :width]
    spot = lax.broadcasted_iota(jnp.int32, cosine.shape, 1)
    leading = spot % (HEAD_DIM // 2) < HEAD_DIM // 4
    pieces = []
    for start in range(0, width, lanes):
        piece = values[:, start : start + lanes]
        other = jnp.where(
            leading,
            pltpu.roll(piece, lanes - HEAD_DIM // 4, 1),
            pltpu.roll(piece, HEAD_DIM // 4, 1),
        )
        pieces.append(piece * cosine + other * sine)
    return jnp.concatenate(pieces, axis=1)


def activate(gate, up):
    capped = jnp.minimum(gate, LIMIT)
    bounded = jnp.clip(up, -LIMIT, LIMIT)
    return (capped * jax.nn.sigmoid(SLOPE * capped) * (bounded + 1.0)).astype(jnp.bfloat16)


def remote(src, dst, sent, landed, ep, tp):
    return pltpu.make_async_remote_copy(
        src_ref=src,
        dst_ref=dst,
        send_sem=sent,
        recv_sem=landed,
        device_id=(ep, tp),
        device_id_type=pl.DeviceIdType.MESH,
    )


def exchange(
    n,
    t,
    x_hbm,
    gain_hbm,
    logit_hbm,
    route_hbm,
    mixer_hbm,
    mixer_gain_hbm,
    frequency_hbm,
    sink_hbm,
    wq_hbm,
    wk_hbm,
    wv_hbm,
    wo_hbm,
    wg_hbm,
    wu_hbm,
    wd_hbm,
    mixer_hbm_out,
    expert_hbm_out,
    mixer_out,
    expert_out,
    gain_ref,
    logit_ref,
    route_ref,
    mixer_gain_ref,
    frequency_ref,
    sink_ref,
    x_ref,
    mixer_ref,
    tokens,
    hidden,
    heads,
    shares,
    half_out,
    half_in,
    result,
    returned,
    kept_half,
    scales,
    cosine_ref,
    sine_ref,
    lent,
    queries,
    around,
    wq,
    wk,
    wv,
    wo,
    wg,
    wu,
    wd,
    local_sem,
    out_sem,
    token_recv,
    up_send,
    down_send,
    core_send,
    hidden_send,
    hidden_recv,
    pass_send,
    head_send,
    head_recv,
    head_pass_send,
    edge_send,
    edge_recv,
    lent_send,
    lent_recv,
    share_send,
    share_recv,
    half_send,
    half_recv,
    result_send,
    result_recv,
):
    ep, tp = lax.axis_index("ep"), lax.axis_index("tp")
    chips = n // 2
    z, core = ep // 2, ep % 2
    partner = 2 * z + 1 - core
    rows = x_ref.shape[0]
    size = rows // SPLIT
    pair = 2 * size
    part = wg.shape[1]
    length = mixer_ref.shape[0]
    kept = wk.shape[1]
    spread = wq.shape[1]
    square = t == 4
    direct = (1, 2) if square else tuple(range(1, t))

    def peer(k):
        if not square:
            return lax.rem(tp + k, t)
        return lax.rem(tp + (k // 2) * 2 + (k % 2) * (1 - 2 * (tp % 2)) + t, t)

    def block(index, size):
        return pl.ds(pl.multiple_of(index * size, size), size)

    loads = [
        pltpu.make_async_copy(a, b, local_sem.at[i])
        for i, (a, b) in enumerate((
            (x_hbm, x_ref),
            (wg_hbm, wg),
            (wu_hbm, wu),
            (mixer_hbm, mixer_ref),
            (wk_hbm, wk),
            (wv_hbm, wv),
            (wq_hbm, wq),
            (wd_hbm, wd),
            (wo_hbm, wo),
            (frequency_hbm, frequency_ref),
            (logit_hbm, logit_ref),
            (route_hbm, route_ref),
            (gain_hbm, gain_ref),
            (mixer_gain_hbm, mixer_gain_ref),
            (sink_hbm, sink_ref),
        ))
    ]
    for load in loads[9:] + loads[:9]:
        load.start()

    barrier = pltpu.get_barrier_semaphore()
    for k in range(1, n):
        pl.semaphore_signal(
            barrier,
            inc=1,
            device_id=(lax.rem(ep + k, n), tp),
            device_id_type=pl.DeviceIdType.MESH,
        )
    for k in range(1, t):
        pl.semaphore_signal(
            barrier,
            inc=1,
            device_id=(ep, peer(k)),
            device_id_type=pl.DeviceIdType.MESH,
        )

    for load in loads[9:]:
        load.wait()
    logits = logit_ref[...]
    raised = jnp.exp(logits - jnp.max(logits, axis=0, keepdims=True))
    chances = raised / jnp.sum(raised, axis=0, keepdims=True)
    number = lax.broadcasted_iota(jnp.int32, (n, rows), 0)
    share = jnp.zeros((n, rows), jnp.float32)
    for k in range(TOP_K):
        share += jnp.where(route_ref[k : k + 1, :] == number, chances[k : k + 1, :], 0.0)
    shares[ep] = share

    lanes = 2 * HEAD_DIM
    spot = lax.broadcasted_iota(jnp.int32, (length, lanes), 1)
    token = ep * length + lax.broadcasted_iota(jnp.int32, (length, lanes), 0)
    turn = jnp.where(spot % HEAD_DIM < HEAD_DIM // 2, token // GRID_W, token % GRID_W)
    turn = turn.astype(jnp.float32) * frequency_ref[...]
    cosine_ref[...] = jnp.cos(turn)
    sine_ref[...] = jnp.sin(turn) * jnp.where(spot % (HEAD_DIM // 2) < HEAD_DIM // 4, -1.0, 1.0)

    loads[0].wait()
    fresh = normalize(x_ref[...], gain_ref[...])
    for sub in range(SPLIT):
        inside = block(2 * (z * SPLIT + sub) + core, size)
        tokens[inside, :] = fresh[sub * size : (sub + 1) * size]

    def unit(place, sub):
        return place * SPLIT + sub

    def token_copy(slot, sent, target):
        piece = tokens.at[block(slot, size)]
        return remote(piece, piece, sent, token_recv.at[slot], target, tp)

    def up_copy(place, sub):
        u = unit(place, sub)
        return token_copy(2 * u + core, up_send.at[u], ep + 2)

    def down_copy(place, sub):
        u = unit(place, sub)
        return token_copy(2 * u + core, down_send.at[u], ep - 2)

    def core_copy(place, sub):
        u = unit(place, sub)
        return token_copy(2 * u + core, core_send.at[0], partner)

    def token_wait(slot):
        token_copy(slot, core_send.at[0], partner).wait_recv()

    def share_copy(k):
        piece = shares.at[ep]
        target = lax.rem(ep + k, n)
        return remote(piece, piece, share_send.at[0], share_recv.at[0], target, tp)

    def share_wait():
        piece = shares.at[pl.ds(0, n - 1)]
        remote(piece, piece, share_send.at[0], share_recv.at[0], partner, tp).wait_recv()

    lowest, highest = z == 0, z == chips - 1

    def spread_own(sub):
        @pl.when(jnp.logical_not(highest))
        def _():
            up_copy(z, sub).start()

        @pl.when(jnp.logical_not(lowest))
        def _():
            down_copy(z, sub).start()

    def hidden_piece(source, u, half):
        return hidden.at[
            block(2 * u + half, size), pl.ds(pl.multiple_of(source * part, part), part)
        ]

    def kind_of(k, half):
        if square and k < 3:
            return jnp.where(half == k - 1, k - 1, 2)
        return 2

    def hidden_copy(source, u, half, k):
        piece = hidden_piece(source, u, half)
        return remote(
            piece,
            piece,
            hidden_send.at[k],
            hidden_recv.at[u, kind_of(k, half)],
            ep,
            peer(k),
        )

    def hidden_forward(u, way):
        source = peer(2 - way)
        piece = hidden_piece(source, u, 1 - way)
        return remote(
            piece,
            piece,
            pass_send.at[way],
            hidden_recv.at[u, 2],
            ep,
            peer(1 + way),
        )

    def hidden_pass(u):
        if square:
            for way in range(2):
                hidden_copy(peer(2 - way), u, 1 - way, 2 - way).wait_recv()
                hidden_forward(u, way).start()

    others = 2 if square else t - 1

    def hidden_wait(u):
        view = hidden.at[pl.ds(0, pair), pl.ds(0, others * part)]
        remote(view, view, hidden_send.at[0], hidden_recv.at[u, 2], ep, peer(1)).wait_recv()

    def head_piece(source, half):
        return heads.at[
            block(half, length // 2),
            pl.ds(pl.multiple_of(source * spread, spread), spread),
        ]

    def head_copy(source, half, k):
        piece = head_piece(source, half)
        return remote(
            piece, piece, head_send.at[k], head_recv.at[kind_of(k, half)], ep, peer(k)
        )

    def head_forward(way):
        source = peer(2 - way)
        piece = head_piece(source, 1 - way)
        return remote(
            piece,
            piece,
            head_pass_send.at[way],
            head_recv.at[2],
            ep,
            peer(1 + way),
        )

    def head_pass():
        if square:
            for way in range(2):
                head_copy(peer(2 - way), 1 - way, 2 - way).wait_recv()
                head_forward(way).start()

    def head_wait():
        view = heads.at[:, pl.ds(0, others * spread)]
        remote(view, view, head_send.at[0], head_recv.at[2], ep, peer(1)).wait_recv()

    def expand(slots):
        span = min(256, part)
        for start in range(0, part, span):
            cut = slice(start, start + span)
            lines = jnp.concatenate([tokens[block(slot, size), :] for slot in slots], axis=0)
            gate = jnp.dot(lines, wg[:, cut], preferred_element_type=jnp.float32)
            up = jnp.dot(lines, wu[:, cut], preferred_element_type=jnp.float32)
            column = pl.ds(pl.multiple_of(tp * part + start, span), span)
            active = activate(gate, up)
            for i, slot in enumerate(slots):
                hidden[block(slot, size), column] = active[i * size : (i + 1) * size]

    def first_half(u):
        token_wait(2 * u + 1 - core)
        expand([2 * u, 2 * u + 1])
        for order in range(2):
            for k in direct:
                hidden_copy(tp, u, order if k != 2 else 1 - order, k).start()

    def first_own(side):
        expand([2 * unit(z, sub) + side for sub in range(SPLIT)])

    def send_own(side):
        for sub in range(SPLIT):
            for k in direct:
                hidden_copy(tp, unit(z, sub), side, k).start()

    pl.semaphore_wait(barrier, n + t - 2)
    for k in range(1, n):
        share_copy(k).start()
    spread_own(0)
    for sub in range(SPLIT):
        core_copy(z, sub).start()
    loads[1].wait()
    loads[2].wait()
    first_own(core)
    send_own(core)

    loads[3].wait()
    normed = normalize(mixer_ref[...], mixer_gain_ref[...])
    own = slice(WINDOW, WINDOW + length)
    for load in loads[4:6]:
        load.wait()
    cosine, sine = cosine_ref[...], sine_ref[...]
    keys = jnp.dot(normed, wk[...], preferred_element_type=jnp.float32)
    around[own, 0:kept] = rotate(keys, cosine, sine).astype(jnp.bfloat16)
    around[own, kept:] = jnp.dot(normed, wv[...], preferred_element_type=jnp.float32).astype(
        jnp.bfloat16
    )

    reach = WINDOW // 2

    def edge_copy(way, part_of):
        source, target = (length, 0) if way == 0 else (WINDOW, WINDOW + length)
        return remote(
            around.at[pl.ds(source + part_of * reach, reach)],
            around.at[pl.ds(target + part_of * reach, reach)],
            edge_send.at[way, part_of],
            edge_recv.at[way, part_of],
            ep + (1 if way == 0 else -1),
            tp,
        )

    def lend_copy(way):
        source = length if way == 0 else WINDOW
        return remote(
            around.at[pl.ds(source + reach, reach)],
            lent,
            edge_send.at[way, 1],
            lent_recv.at[0],
            partner,
            tp,
        )

    def lent_copy(way):
        target = 0 if way == 0 else WINDOW + length
        return remote(
            lent,
            around.at[pl.ds(target + reach, reach)],
            lent_send.at[0],
            edge_recv.at[way, 1],
            partner + (1 if way == 0 else -1),
            tp,
        )

    first, last = ep == 0, ep == n - 1

    crossing = ((core == 1) & jnp.logical_not(highest), (core == 0) & jnp.logical_not(lowest))
    lending = ((core == 0) & jnp.logical_not(highest), (core == 1) & jnp.logical_not(lowest))
    for way in range(2):
        @pl.when(core == way)
        def _():
            for part_of in range(2):
                edge_copy(way, part_of).start()

        @pl.when(crossing[way])
        def _():
            lend_copy(way).start()
            edge_copy(way, 0).start()

    for sub in range(1, SPLIT):
        spread_own(sub)

    @pl.when(first)
    def _():
        around[0:WINDOW, :] = jnp.zeros((WINDOW, around.shape[1]), jnp.bfloat16)

    @pl.when(last)
    def _():
        around[WINDOW + length :, :] = jnp.zeros((WINDOW, around.shape[1]), jnp.bfloat16)

    for sub in range(SPLIT):
        token_wait(2 * unit(z, sub) + 1 - core)
    first_own(1 - core)
    send_own(1 - core)

    for way in range(2):
        @pl.when(lending[way])
        def _():
            lend_copy(way).wait_recv()
            lent_copy(way).start()

    loads[6].wait()
    turned = jnp.dot(normed, wq[...], preferred_element_type=jnp.float32)
    queries[...] = rotate(turned, cosine, sine).astype(jnp.bfloat16)

    def attend(number, carry):
        inside = pl.ds(pl.multiple_of(number * WINDOW, WINDOW), WINDOW)
        seen = pl.ds(pl.multiple_of(number * WINDOW, WINDOW), 3 * WINDOW)
        shape = (WINDOW, 3 * WINDOW)
        line = lax.broadcasted_iota(jnp.int32, shape, 0)
        key = lax.broadcasted_iota(jnp.int32, shape, 1)
        place = ep * length + (number - 1) * WINDOW + key
        allowed = (key >= line) & (key <= line + 2 * WINDOW) & (place >= 0) & (place < n * length)
        group = queries.shape[1] // kept
        allowed = jnp.concatenate([allowed] * group, axis=0)
        for head in range(kept // HEAD_DIM):
            first = head * group
            query = jnp.concatenate(
                [
                    queries[inside, (first + r) * HEAD_DIM : (first + r + 1) * HEAD_DIM]
                    for r in range(group)
                ],
                axis=0,
            )
            sinks = jnp.concatenate(
                [
                    jnp.broadcast_to(sink_ref[:, first + r : first + r + 1], (WINDOW, 1))
                    for r in range(group)
                ],
                axis=0,
            )
            near_keys = around[seen, head * HEAD_DIM : (head + 1) * HEAD_DIM]
            near_values = around[seen, kept + head * HEAD_DIM : kept + (head + 1) * HEAD_DIM]
            scores = lax.dot_general(
                query,
                near_keys,
                (((1,), (1,)), ((), ())),
                preferred_element_type=jnp.float32,
            ) * HEAD_DIM ** (-0.5)
            scores = jnp.where(allowed, scores, -1e30)
            top = jnp.maximum(jnp.max(scores, axis=-1, keepdims=True), sinks)
            weights = jnp.exp(scores - top)
            denominator = jnp.sum(weights, axis=-1, keepdims=True) + jnp.exp(sinks - top)
            share = (weights * (1.0 / denominator)).astype(jnp.bfloat16)
            mixed = jnp.dot(share, near_values, preferred_element_type=jnp.float32)
            mixed = mixed.astype(jnp.bfloat16)
            width = group * HEAD_DIM
            column = pl.ds(pl.multiple_of(tp * spread + first * HEAD_DIM, width), width)
            heads[inside, column] = jnp.concatenate(
                [mixed[r * WINDOW : (r + 1) * WINDOW] for r in range(group)], axis=1
            )
        return carry

    def attention(half):
        for way in range(2):
            @pl.when((half == way) & jnp.logical_not(first if way == 0 else last))
            def _():
                for part_of in range(2):
                    edge_copy(way, part_of).wait_recv()

        count = length // 2 // WINDOW
        lax.fori_loop(half * count, (half + 1) * count, attend, 0)
        for k in direct:
            head_copy(tp, half, k).start()

    def half_copy(u):
        return remote(
            half_out.at[u], half_in.at[u], half_send.at[0], half_recv.at[u], partner, tp
        )

    def result_copy(u, source):
        return remote(
            result.at[u],
            returned.at[source, u % SPLIT],
            result_send.at[0],
            result_recv.at[u % SPLIT],
            2 * (u // SPLIT) + core,
            tp,
        )

    def spread_shares(slot, carry):
        line = shares[slot, pl.ds(ep, 1), :]
        column = jnp.transpose(jnp.broadcast_to(line, (rows, rows)))
        for sub in range(SPLIT):
            inside = block(2 * unit(slot // 2, sub) + slot % 2, size)
            scales[inside, :] = column[sub * size : (sub + 1) * size]
        return carry

    def second_half(u):
        hidden_wait(u)
        inside = block(u, pair)
        total = jnp.dot(hidden[inside, :], wd[...], preferred_element_type=jnp.float32)
        column = scales[inside, :]
        kept_half[u] = jnp.concatenate(
            [total[:, i : i + rows] * column for i in range(0, total.shape[1], rows)], axis=1
        )
        half_out[u] = kept_half[u, block(1 - core, size), :].astype(jnp.bfloat16)
        half_copy(u).start()

    def combine(u):
        half_copy(u).wait_recv()
        total = kept_half[u, block(core, size), :] + half_in[u].astype(jnp.float32)
        result[u] = total.astype(jnp.bfloat16)

    def sides(hop, action):
        def side(k, carry):
            place = z + (2 * k - 1) * hop

            @pl.when((place >= 0) & (place < chips))
            def _():
                action(place, k)

            return carry

        lax.fori_loop(0, 2, side, 0)

    def arrive(hop, sub):
        below, above = z - hop, z + hop

        @pl.when(below >= 0)
        def _():
            token_wait(2 * unit(below, sub) + core)

            @pl.when(jnp.logical_not(highest))
            def _():
                up_copy(below, sub).start()

            core_copy(below, sub).start()

        @pl.when(above < chips)
        def _():
            token_wait(2 * unit(above, sub) + core)

            @pl.when(jnp.logical_not(lowest))
            def _():
                down_copy(above, sub).start()

            core_copy(above, sub).start()

    steps = (chips - 1) * SPLIT

    def one(index, action):
        hop, sub = 1 + index // SPLIT, index % SPLIT
        below, above = z - hop, z + hop

        @pl.when((below >= 0) | (above < chips))
        def _():
            action(unit(jnp.where(below >= 0, below, above), sub))

    def two(index, action):
        hop, sub = 1 + index // SPLIT, index % SPLIT
        below, above = z - hop, z + hop

        @pl.when((below >= 0) & (above < chips))
        def _():
            action(unit(above, sub))

    def deliver(u):
        combine(u)
        result_copy(u, z).start()

    ending = lowest | highest
    look = jnp.where(ending, EARLY, LATE)

    def own_units(action):
        for sub in range(SPLIT):
            action(unit(z, sub))

    mixer_store = pltpu.make_async_copy(mixer_out, mixer_hbm_out, out_sem.at[SPLIT])

    def expert_store(sub):
        inside = pl.ds(sub * size, size)
        return pltpu.make_async_copy(expert_out.at[inside], expert_hbm_out.at[inside], out_sem.at[sub])

    def project():
        head_wait()
        mixer_out[...] = jnp.dot(heads[...], wo[...], preferred_element_type=jnp.float32).astype(
            jnp.bfloat16
        )
        mixer_store.start()

    def drain(u, carry):
        place, sub = u // SPLIT, u % SPLIT

        @pl.when((place <= z) & jnp.logical_not(highest))
        def _():
            up_copy(place, sub).wait_send()

        @pl.when((place >= z) & jnp.logical_not(lowest))
        def _():
            down_copy(place, sub).wait_send()

        return carry

    def sent(view, semaphore):
        remote(view, view, semaphore, semaphore, partner, tp).wait_send()

    def column(buffer, count, extent):
        return buffer.at[pl.ds(0, count), pl.ds(0, extent)]

    def drain_early():
        lax.fori_loop(0, units, drain, 0)
        sent(tokens.at[pl.ds(0, rows * chips)], core_send.at[0])
        sent(shares.at[pl.ds(0, n - 1)], share_send.at[0])
        for way in range(2):
            @pl.when((core == way) | crossing[way])
            def _():
                for part_of in range(2):
                    edge_copy(way, part_of).wait_send()

            @pl.when(lending[way])
            def _():
                lent_copy(way).wait_send()

    def drain_late():
        sent(half_out, half_send.at[0])
        sent(result.at[pl.ds(0, units - SPLIT)], result_send.at[0])
        for k in direct:
            sent(column(hidden, n * rows, part), hidden_send.at[k])
            sent(column(heads, length, spread), head_send.at[k])
        if square:
            for way in range(2):
                sent(column(hidden, chips * rows, part), pass_send.at[way])
                head_forward(way).wait_send()

    units = chips * SPLIT

    def step(index, carry):
        hop, sub = 1 + index // SPLIT, index % SPLIT
        arrive(hop, sub)
        sides(hop, lambda place, k: first_half(unit(place, sub)))

        @pl.when(index == 0)
        def _():
            for own_sub in range(1, SPLIT):
                hidden_pass(unit(z, own_sub))

        @pl.when(index > 0)
        def _():
            one(index - 1, hidden_pass)

        @pl.when(index > 1)
        def _():
            two(index - 2, hidden_pass)

        @pl.when((index >= look) & (index < look + 2))
        def _():
            attention(jnp.where(highest, 1 - (index - look), index - look))

        @pl.when((index == 3) & ending)
        def _():
            head_pass()

        @pl.when(index > 2)
        def _():
            one(index - 3, deliver)

        @pl.when(index > 1)
        def _():
            one(index - 2, second_half)

        @pl.when(index > 3)
        def _():
            two(index - 4, deliver)

        @pl.when(index > 2)
        def _():
            two(index - 3, second_half)

        return carry

    loads[7].wait()
    share_wait()
    lax.fori_loop(0, n, spread_shares, 0)
    hidden_pass(unit(z, 0))
    lax.fori_loop(0, steps, step, 0)
    loads[8].wait()
    second_half(unit(z, 0))
    one(steps - 1, hidden_pass)
    two(steps - 2, hidden_pass)
    two(steps - 1, hidden_pass)
    for sub in range(1, SPLIT):
        second_half(unit(z, sub))
    one(steps - 3, deliver)
    two(steps - 4, deliver)
    @pl.when(ending)
    def _():
        project()

    drain_early()
    one(steps - 2, second_half)
    two(steps - 3, second_half)
    one(steps - 2, deliver)
    two(steps - 3, deliver)

    one(steps - 1, second_half)
    two(steps - 2, second_half)
    two(steps - 1, second_half)
    one(steps - 1, deliver)
    two(steps - 2, deliver)
    two(steps - 1, deliver)

    @pl.when(jnp.logical_not(ending))
    def _():
        head_pass()
        project()

    own_units(combine)
    drain_late()

    for sub in range(SPLIT):
        total = result[unit(z, sub)].astype(jnp.float32)
        view = result.at[pl.ds(0, chips - 1)]
        remote(view, view, result_send.at[0], result_recv.at[sub], partner, tp).wait_recv()
        for k in range(1, chips):
            source = lax.rem(z + k, chips)
            total += returned[source, sub].astype(jnp.float32)
        expert_out[sub * size : (sub + 1) * size, :] = total.astype(jnp.bfloat16)
        expert_store(sub).start()

    for sub in range(SPLIT):
        expert_store(sub).wait()
    mixer_store.wait()


def settle(first_in, second_in, first_out, second_out, first, second, semaphore):
    taken = [
        pltpu.make_async_copy(a, b, semaphore.at[i])
        for i, (a, b) in enumerate(((first_in, first), (second_in, second)))
    ]
    given = [
        pltpu.make_async_copy(a, b, semaphore.at[2 + i])
        for i, (a, b) in enumerate(((first, first_out), (second, second_out)))
    ]
    for copy in taken:
        copy.start()
    for i in (1, 0):
        taken[i].wait()
        given[i].start()
    for copy in given:
        copy.wait()


def shards(
    mixer_input,
    mixer_gain,
    query_weight,
    key_weight,
    value_weight,
    output_weight,
    sink_logit,
    expert_input,
    expert_gain,
    routes,
    route_logits,
    gate_weight,
    up_weight,
    down_weight,
):
    tokens = mixer_input.shape[0]
    lanes = 2 * HEAD_DIM
    quarter = HEAD_DIM // 4
    spot = np.arange(lanes) % quarter
    frequency = (BASE ** (-spot.astype(np.float32) / np.float32(quarter))).astype(np.float32)[None]
    experts = lax.axis_size("ep")
    parts = lax.axis_size("tp")
    rows, width = expert_input.shape
    part = gate_weight.shape[2]
    vmem = pl.BlockSpec(memory_space=pltpu.VMEM)
    outside = pl.BlockSpec(memory_space=pltpu.HBM)
    chips = experts // 2
    dma = pltpu.SemaphoreType.DMA
    columns = down_weight.shape[2]
    spread = query_weight.shape[1]
    half = jnp.bfloat16
    size, units = rows // SPLIT, chips * SPLIT
    results = pl.pallas_call(
        functools.partial(exchange, experts, parts),
        out_shape=(
            jax.ShapeDtypeStruct((tokens, output_weight.shape[1]), half),
            jax.ShapeDtypeStruct((rows, columns), half),
        ),
        in_specs=[outside] * 15,
        out_specs=(outside, outside),
        scratch_shapes=[
            pltpu.VMEM((tokens, output_weight.shape[1]), half),
            pltpu.VMEM((rows, columns), half),
            pltpu.VMEM((1, width), jnp.float32),
            pltpu.VMEM((TOP_K, rows), jnp.float32),
            pltpu.VMEM((TOP_K, rows), jnp.int32),
            pltpu.VMEM((1, width), jnp.float32),
            pltpu.VMEM((1, lanes), jnp.float32),
            pltpu.VMEM((1, sink_logit.shape[0]), jnp.float32),
            pltpu.VMEM((rows, width), half),
            pltpu.VMEM(mixer_input.shape, half),
            pltpu.VMEM((experts * rows, width), half),
            pltpu.VMEM((experts * rows, parts * part), half),
            pltpu.VMEM((tokens, parts * spread), half),
            pltpu.VMEM((experts, experts, rows), jnp.float32),
            pltpu.VMEM((units, size, columns), half),
            pltpu.VMEM((units, size, columns), half),
            pltpu.VMEM((units, size, columns), half),
            pltpu.VMEM((chips, SPLIT, size, columns), half),
            pltpu.VMEM((units, 2 * size, columns), jnp.float32),
            pltpu.VMEM((experts * rows, rows), jnp.float32),
            pltpu.VMEM((tokens, lanes), jnp.float32),
            pltpu.VMEM((tokens, lanes), jnp.float32),
            pltpu.VMEM((WINDOW // 2, 2 * key_weight.shape[1]), half),
            pltpu.VMEM((tokens, spread), half),
            pltpu.VMEM((tokens + 2 * WINDOW, 2 * key_weight.shape[1]), half),
            pltpu.VMEM(query_weight.shape, half),
            pltpu.VMEM(key_weight.shape, half),
            pltpu.VMEM(value_weight.shape, half),
            pltpu.VMEM(output_weight.shape, half),
            pltpu.VMEM(gate_weight.shape[1:], half),
            pltpu.VMEM(up_weight.shape[1:], half),
            pltpu.VMEM(down_weight.shape[1:], half),
            dma((15,)),
            dma((SPLIT + 1,)),
            dma((2 * units,)),
            dma((units,)),
            dma((units,)),
            dma((1,)),
            dma((parts,)),
            dma((units, 3)),
            dma((2,)),
            dma((parts,)),
            dma((3,)),
            dma((2,)),
            dma((2, 2)),
            dma((2, 2)),
            dma((1,)),
            dma((1,)),
            dma((1,)),
            dma((1,)),
            dma((1,)),
            dma((units,)),
            dma((1,)),
            dma((SPLIT,)),
        ],
        compiler_params=pltpu.CompilerParams(
            collective_id=0, has_side_effects=True, vmem_limit_bytes=60 * 1024 * 1024
        ),
    )(
        expert_input,
        expert_gain.reshape(1, -1),
        route_logits.T,
        routes.T,
        mixer_input,
        mixer_gain.reshape(1, -1),
        jnp.asarray(frequency),
        sink_logit.reshape(1, -1),
        query_weight,
        key_weight,
        value_weight,
        output_weight,
        gate_weight[0],
        up_weight[0],
        down_weight[0],
    )
    return pl.pallas_call(
        settle,
        out_shape=tuple(jax.ShapeDtypeStruct(r.shape, r.dtype) for r in results),
        in_specs=[outside, outside],
        out_specs=(outside, outside),
        scratch_shapes=[pltpu.VMEM(r.shape, r.dtype) for r in results] + [dma((4,))],
    )(*results)


def solution(mesh):
    return jax.shard_map(
        shards,
        mesh=mesh,
        in_specs=(
            P("ep", None),
            P(),
            P(None, "tp"),
            P(None, "tp"),
            P(None, "tp"),
            P(None, "tp"),
            P("tp"),
            P("ep", None),
            P(),
            P("ep", None),
            P("ep", None),
            P("ep", None, "tp"),
            P("ep", None, "tp"),
            P("ep", None, "tp"),
        ),
        out_specs=(P("ep", "tp"), P("ep", "tp")),
        check_vma=False,
    )
```
